32 devices in a mesh: gr: 2 (over x), fs: 8 (over z, y), tp: 2 (over core).
Axes of the slice: x: 2, y: 2, z: 4, core: 2. Of those that a mesh axis runs over, the one named last changes fastest.
Arguments:
- prompt_tokens: bfloat16 [4608, 2048], P(('gr', 'fs', 'tp')), may hold values from -6 to 6
- up_master: float32 [2048, 8192], P(('gr', 'fs'), 'tp'), may hold values from -0.125 to 0.125
- down_master: float32 [2048, 8192], P(('gr', 'fs'), 'tp'), may hold values from -0.0625 to 0.0625
- norm_gain: float32 [2048], P(('gr', 'fs')), may hold values from 0.1 to 1.9
Outputs:
- sampler_up: bfloat16 [2048, 8192], P(None, ('gr', 'tp'))
- sampler_down: bfloat16 [2048, 8192], P(None, ('gr', 'tp'))
- prompt_out: bfloat16 [4608, 2048], P(('gr', 'fs', 'tp'))
The draws below stay inside these ranges and needn't reach their ends.
All inputs are finite; a program needn't handle non-finite values.
Results may differ from the reference program's by a relative error of at most 0.009.
Values may be sent and summed in bfloat16 or wider, within the bound.
A program may use at most 128 MiB of HBM per device.

```python
import jax
import jax.numpy as jnp
from jax import lax

D = 2048
FF = 8192
TOKENS = 4608
N_GR = 2
N_TP = 2


def steps_of(stream_key, dims, shards, low, high):
    level = 1.0
    for dim, parts in shards:
        draws = jax.random.uniform(jax.random.fold_in(jax.random.fold_in(stream_key, 6), dim), (parts,), jnp.float32, low / len(shards), high / len(shards))
        level = level * jnp.repeat(jnp.exp(draws), dims[dim] // parts).reshape((-1,) + (1,) * (len(dims) - 1 - dim))
    return level


def gaussian(own_key, shape, scale, reach, split=(), kind=jnp.bfloat16):
    drawn = jax.random.normal(own_key, shape, jnp.float32) * scale
    if len(split) > 0:
        drawn = steps_of(own_key, shape, split, -0.22, 0.18) * drawn
    return jnp.clip(drawn, min=-reach, max=reach).astype(kind)


def setup_inputs(seed: int = 0) -> dict:
    streams_of = jax.random.split(jax.random.key(seed), 5)
    prompt_tokens = gaussian(streams_of[0], (TOKENS, D), 1.0, 6.0, ((0, 32),))
    up_master = gaussian(streams_of[1], (D, FF), D ** -0.5, 0.125, ((0, 16), (1, 2)), jnp.float32)
    down_master = gaussian(streams_of[2], (D, FF), FF ** -0.5, 0.0625, ((0, 16), (1, 2)), jnp.float32)
    norm_gain = jnp.clip(1.0 + 0.18 * jax.random.normal(streams_of[3], (D,), jnp.float32), 0.1, 1.9)
    return {"prompt_tokens": prompt_tokens, "up_master": up_master, "down_master": down_master, "norm_gain": norm_gain}


def reference(prompt_tokens, up_master, down_master, norm_gain):
    sampler_up = (norm_gain[:, None] * up_master).astype(jnp.bfloat16)
    sampler_down = down_master.astype(jnp.bfloat16)
    values = prompt_tokens.astype(jnp.float32)
    center = lax.optimization_barrier(jnp.mean(values, axis=-1, keepdims=True))
    spread = lax.optimization_barrier(jnp.mean(jnp.square(values - center), axis=-1, keepdims=True))
    normed = ((values - center) * lax.rsqrt(spread + 1e-05)).astype(jnp.bfloat16)
    width = FF // (N_GR * N_TP)

    def block_step(total, index):
        start = (index * width).astype(jnp.int32)
        up_block = lax.dynamic_slice_in_dim(sampler_up, start, width, 1)
        down_block = lax.dynamic_slice_in_dim(sampler_down, start, width, 1)
        lifted = jax.nn.relu(jnp.dot(normed, up_block, preferred_element_type=jnp.float32))
        hidden = (lifted * lifted).astype(jnp.bfloat16)
        partial_value = lax.dot_general(hidden, down_block, (((1,), (1,)), ((), ())), preferred_element_type=jnp.float32)
        partial_value = lax.optimization_barrier(partial_value.astype(jnp.bfloat16)).astype(jnp.float32)
        return (total + partial_value, None)
    total, unused = lax.scan(block_step, jnp.zeros((TOKENS, D), jnp.float32), jnp.arange(N_GR * N_TP, dtype=jnp.int32))
    return (sampler_up, sampler_down, total.astype(jnp.bfloat16))
```

```python
import functools

import jax
import jax.numpy as jnp
from jax import lax
from jax.experimental import pallas as pl
from jax.experimental.pallas import tpu as pltpu
from jax.sharding import PartitionSpec as P

MESH = pl.DeviceIdType.MESH
CHUNK = 32
TILE = 256
SPLIT = 4


def pair_first(count):
    return (count * 5 // 32, (count * 5 + 31) // 32)


def kernel(G, F, T, tok_in, gain_in, up_in, down_in, up_full, down_full, part,
           wide, narrow, raw, nrm, hid, stage,
           recv, dup, cross, cross_down, sendl, sendr, sendy, send0, tok_recv, tok_send,
           part_recv, part_send, local_sem, load_sem):
    gr, f, tp = lax.axis_index("gr"), lax.axis_index("fs"), lax.axis_index("tp")
    full = (up_full, down_full)
    A = F // 2
    a, y = f // 2, f % 2
    mate = a * 2 + 1 - y
    R = up_in.shape[0]
    D, W = up_full.shape
    tok = tok_in.shape[0]
    CH = min(CHUNK, R)
    C = R // CH
    NQ = G * C
    PAIR_FIRST = pair_first(NQ)
    K = G * T
    k = gr * T + tp
    weights = (up_in, down_in)

    def at_k(kk):
        return (kk // T, f, kk % T)

    def load(m, c):
        rows = pl.ds(c * CH, CH)
        return pltpu.make_async_copy(weights[m].at[rows], wide.at[m, rows], load_sem.at[m, c])

    barrier = pltpu.get_barrier_semaphore()

    @pl.when(a > 0)
    def _():
        pl.semaphore_signal(barrier, inc=1, device_id=(gr, f - 2, tp), device_id_type=MESH)

    @pl.when(a < A - 1)
    def _():
        pl.semaphore_signal(barrier, inc=1, device_id=(gr, f + 2, tp), device_id_type=MESH)
    pl.semaphore_signal(barrier, inc=1, device_id=(gr, mate, tp), device_id_type=MESH)
    for d in range(1, K):
        pl.semaphore_signal(barrier, inc=1, device_id=at_k((k + d) % K), device_id_type=MESH)

    token_load = pltpu.make_async_copy(tok_in, raw, local_sem.at[0])
    for c in range(C):
        load(0, c).start()
    for c in range(C):
        load(1, c).start()
    token_load.start()

    def rows_of(origin, g, c):
        return pl.ds(pl.multiple_of(g * (F * R) + origin * R + c * CH, CH), CH)

    home = k // G == tp

    def cast(m, c):
        rows = pl.ds(c * CH, CH)
        load(m, c).wait()
        value = wide[m, rows, :]
        if m == 0:
            value = value * column[c * CH:(c + 1) * CH]
        value = value.astype(jnp.bfloat16)
        narrow[m, rows, :] = value
        for b in range(G):
            @pl.when(tp * G + b == k)
            def _():
                full[m][rows_of(f, gr, c), :] = value[:, b * W:(b + 1) * W]

    def hand(m, b, c):
        kk = tp * G + b
        q = ((gr - kk // T + G) % G) * C + c

        @pl.when(kk != k)
        def _():
            copy = pltpu.make_async_remote_copy(
                src_ref=narrow.at[m, pl.ds(c * CH, CH), pl.ds(b * W, W)],
                dst_ref=full[m].at[rows_of(f, gr, c)],
                send_sem=send0.at[0], recv_sem=recv.at[m, a, q],
                device_id=at_k(kk), device_id_type=MESH)
            copy.start()

    mine = pl.ds(pl.multiple_of(k * tok, 16), tok)

    def tokens():
        for d in range(1, K):
            pltpu.make_async_remote_copy(
                src_ref=nrm.at[mine], dst_ref=nrm.at[mine],
                send_sem=tok_send.at[0], recv_sem=tok_recv.at[0],
                device_id=at_k((k + d) % K), device_id_type=MESH).start()

    def normalize(i, carry):
        values = raw[pl.ds(pl.multiple_of(i * 16, 16), 16), :].astype(jnp.float32)
        center = jnp.mean(values, axis=-1, keepdims=True)
        moved = values - center
        spread = jnp.mean(jnp.square(moved), axis=-1, keepdims=True)
        nrm[pl.ds(pl.multiple_of(k * tok + i * 16, 16), 16), :] = (
            moved * lax.rsqrt(spread + 1e-05)).astype(jnp.bfloat16)
        return carry

    rowed = lax.broadcasted_iota(jnp.int32, (R, R), 0) == lax.broadcasted_iota(jnp.int32, (R, R), 1)
    column = jnp.sum(jnp.where(rowed, gain_in[...], 0.0), axis=1, keepdims=True)

    for c in range(C):
        cast(0, c)
    pl.semaphore_wait(barrier, K + (a > 0).astype(jnp.int32) + (a < A - 1).astype(jnp.int32))
    for c in range(C):
        for b in range(G):
            hand(0, b, c)

    def chunk(m, origin, q):
        return full[m].at[rows_of(origin, (gr + q // C) % G, q % C)]

    def landing(m, origin_a, side, q):
        if side == "line":
            return recv.at[m, origin_a, q]
        if side == "pair":
            return dup.at[m, origin_a, q]
        return cross.at[0] if m == 0 else cross_down.at[origin_a, q // C]

    def send(m, origin, q, sem, side, target):
        ref = chunk(m, origin, q)
        pltpu.make_async_remote_copy(
            src_ref=ref, dst_ref=ref, send_sem=sem.at[0], recv_sem=landing(m, origin // 2, side, q),
            device_id=(gr, target, tp), device_id_type=MESH).start()

    def await_rows(ref, count, sem):
        if count > 0:
            rows = ref.at[pl.ds(0, count)]
            pltpu.make_async_copy(rows, rows, sem).wait()

    def arrived(m, origin, q, side="line"):
        ref = chunk(m, origin, q)
        pltpu.make_async_copy(ref, ref, landing(m, origin // 2, side, q)).wait()

    def left(m, origin, q, side="line"):
        @pl.when(a > 0)
        def _():
            send(m, origin, q, sendl, side, f - 2)

    def right(m, origin, q, side="line"):
        @pl.when(a < A - 1)
        def _():
            send(m, origin, q, sendr, side, f + 2)

    def loop(low, high, step):
        def go(i, carry):
            step(i)
            return carry
        if high > low:
            lax.fori_loop(low, high, go, 0)

    def own(m):
        def go(side):
            def step(q):
                @pl.when(jnp.logical_or(q >= C, jnp.logical_not(home)))
                def _():
                    arrived(m, f, q)
                left(m, f, q)
                right(m, f, q)
                send(m, f, q, sendy, side, mate)
            return step
        pf = PAIR_FIRST[m]
        loop(0, pf, go("pair"))
        if m == 0:
            loop(pf, NQ, go("cross"))
        else:
            loop(C, NQ, go("cross"))
            loop(pf, C, go("cross"))

    def mated(m):
        def step(q):
            arrived(m, mate, q, "pair")
            left(m, mate, q, "pair")
            right(m, mate, q, "pair")
        loop(0, PAIR_FIRST[m], step)

    def line(m, s, between=None, eager=None):
        below, above = a - 1 - s, a + 1 + s

        def pass_on(origin, side, q, onward, across):
            arrived(m, origin, q, side)
            onward(m, origin, q, side)
            if across:
                send(m, origin, q, sendy, "cross", mate)

        def both(side, across):
            def step(q):
                mine_y = y if side == "line" else 1 - y

                @pl.when(below >= 0)
                def _():
                    pass_on(below * 2 + mine_y, side, q, right, across)

                @pl.when(above < A)
                def _():
                    pass_on(above * 2 + mine_y, side, q, left, across)
            return step

        pf = PAIR_FIRST[m]
        loop(0, pf, both("line", False))
        if m == 0:
            loop(pf, NQ, both("line", True))
        else:
            loop(C, NQ, both("line", True))
            if between is not None:
                between()
            loop(pf, C, both("line", True))
        if eager is not None:
            eager()
        loop(0, pf, both("pair", False))

    def settle_down(origin_a, gi):
        if C > PAIR_FIRST[1]:
            @pl.when(gi == 0)
            def _():
                await_rows(down_full, (C - PAIR_FIRST[1]) * CH, cross_down.at[origin_a, 0])

        @pl.when(gi > 0)
        def _():
            await_rows(down_full, C * CH, cross_down.at[origin_a, gi])

    own(0)
    token_load.wait()
    lax.fori_loop(0, tok // 16, normalize, 0)
    for c in range(C):
        cast(1, c)
        for b in range(G):
            hand(1, b, c)
    tokens()
    mated(0)
    loop(0, A - 2, lambda s: line(0, s))
    own(1)
    line(0, A - 2)
    mated(1)
    line(1, 0)

    await_rows(up_full, A * (NQ - PAIR_FIRST[0]) * CH, cross.at[0])
    await_rows(nrm, (K - 1) * tok, tok_recv.at[0])

    tile = min(TILE, W)

    def lift(j):
        columns = pl.ds(pl.multiple_of(j * tile, tile), tile)
        lifted = jnp.maximum(jnp.dot(nrm[...], up_full[:, columns], preferred_element_type=jnp.float32), 0.0)
        hid[:, columns] = (lifted * lifted).astype(jnp.bfloat16)
    loop(0, W // tile, lift)

    def part_copy(d, block):
        target = (k + d) % K
        return pltpu.make_async_remote_copy(
            src_ref=stage.at[block, pl.ds(pl.multiple_of(target * tok, 16), tok)],
            dst_ref=part.at[d - 1, block],
            send_sem=part_send.at[0], recv_sem=part_recv.at[0],
            device_id=at_k(target), device_id_type=MESH)

    def lower(origin_a, gi):
        settle_down(origin_a, gi)
        g = (gr + gi) % G
        block = origin_a * G + g
        rows = pl.ds(pl.multiple_of(g * (F * R) + origin_a * (2 * R), 2 * R), 2 * R)
        value = lax.dot_general(hid[...], down_full[rows, :], (((1,), (1,)), ((), ())),
                                preferred_element_type=jnp.float32)
        stage[block] = value.astype(jnp.bfloat16)
        part[K - 1, block] = stage[block, mine]
        for d in range(1, K):
            part_copy(d, block).start()

    def lower_ring(s, low=0, high=G):
        @pl.when(a - 1 - s >= 0)
        def _():
            loop(low, high, lambda i: lower(a - 1 - s, G - 1 - i))

        @pl.when(a + 1 + s < A)
        def _():
            loop(low, high, lambda i: lower(a + 1 + s, G - 1 - i))

    loop(0, G, lambda i: lower(a, G - 1 - i))
    loop(1, A - 2, lambda s: line(1, s, between=lambda: lower_ring(s - 1)))
    line(1, A - 2, between=lambda: lower_ring(A - 3), eager=lambda: lower_ring(A - 2, 0, G - 1))
    lower_ring(A - 2, G - 1, G)

    await_rows(part, K - 1, part_recv.at[0])
    await_rows(part, K - 1, part_send.at[0])
    await_rows(nrm, (K - 1) * tok, tok_send.at[0])
    pairs = sum(PAIR_FIRST)
    await_rows(up_full, 2 * NQ * CH, sendy.at[0])
    for _ in range(A - 1):
        await_rows(up_full, (2 * NQ - pairs) * CH, sendy.at[0])

    def drain(sem, rows):
        def step(i, carry):
            await_rows(up_full, rows, sem.at[0])
            return carry
        return step
    lax.fori_loop(0, jnp.where(a > 0, A - a, 0), drain(sendl, (2 * NQ + pairs) * CH), 0)
    lax.fori_loop(0, jnp.where(a < A - 1, a + 1, 0), drain(sendr, (2 * NQ + pairs) * CH), 0)
    lax.fori_loop(0, jnp.where(home, G - 1, G), drain(send0, 2 * R), 0)


def finish(G, F, up_held, down_held, parts, up_out, down_out, out_ref, sems):
    def out(m, i):
        source, target = ((up_held, up_out), (down_held, down_out))[m]
        size = source.shape[0] // SPLIT
        rows = pl.ds(i * size, size)
        return pltpu.make_async_copy(source.at[rows], target.at[rows], sems.at[m, i])

    for m in range(2):
        for i in range(SPLIT):
            out(m, i).start()
    K, blocks, _, wide = parts.shape
    D = out_ref.shape[1]
    for block in range(blocks):
        total = parts[0, block].astype(jnp.float32)
        for i in range(1, K):
            total += parts[i, block].astype(jnp.float32)
        begin = (block % G) * (D // G) + (block // G) * wide
        out_ref[:, begin:begin + wide] = total.astype(jnp.bfloat16)
    for m in range(2):
        for i in range(SPLIT):
            out(m, i).wait()


def body(G, F, T, prompt_tokens, up_master, down_master, norm_gain):
    R, width = up_master.shape
    tok = prompt_tokens.shape[0]
    D, W = R * G * F, width // G
    A, K = F // 2, G * T
    C = R // min(CHUNK, R)
    NQ = G * C
    bf16 = jnp.bfloat16
    any_space = pl.BlockSpec(memory_space=pl.ANY)
    vmem_space = pl.BlockSpec(memory_space=pltpu.VMEM)
    dma = pltpu.SemaphoreType.DMA
    up_held, down_held, parts = pl.pallas_call(
        functools.partial(kernel, G, F, T),
        name="handoff",
        out_shape=(
            pltpu.MemorySpace.VMEM((D, W), bf16),
            pltpu.MemorySpace.VMEM((D, W), bf16),
            pltpu.MemorySpace.VMEM((K, A * G, tok, 2 * R), bf16),
        ),
        in_specs=[any_space, vmem_space, any_space, any_space],
        out_specs=(vmem_space,) * 3,
        scratch_shapes=[
            pltpu.VMEM((2, R, width), jnp.float32),
            pltpu.VMEM((2, R, width), bf16),
            pltpu.VMEM((tok, D), bf16),
            pltpu.VMEM((K * tok, D), bf16),
            pltpu.VMEM((K * tok, W), bf16),
            pltpu.VMEM((A * G, K * tok, 2 * R), bf16),
            dma((2, A, NQ)), dma((2, A, max(1, max(pair_first(NQ))))), dma((1,)), dma((A, G)),
            dma((1,)), dma((1,)), dma((1,)), dma((1,)), dma((1,)), dma((1,)),
            dma((1,)), dma((1,)), dma((1,)), dma((2, C)),
        ],
        compiler_params=pltpu.CompilerParams(
            collective_id=0, has_side_effects=True, vmem_limit_bytes=41 * 1024 * 1024),
    )(prompt_tokens, norm_gain.reshape(1, R), up_master, down_master)
    return pl.pallas_call(
        functools.partial(finish, G, F),
        name="finish",
        out_shape=(
            jax.ShapeDtypeStruct((D, W), bf16),
            jax.ShapeDtypeStruct((D, W), bf16),
            jax.ShapeDtypeStruct((tok, D), bf16),
        ),
        in_specs=[vmem_space] * 3,
        out_specs=(any_space, any_space, vmem_space),
        scratch_shapes=[dma((2, SPLIT))],
        compiler_params=pltpu.CompilerParams(vmem_limit_bytes=16 * 1024 * 1024),
    )(up_held, down_held, parts)


def solution(mesh):
    placed = (
        P(("gr", "fs", "tp"), None),
        P(("gr", "fs"), "tp"),
        P(("gr", "fs"), "tp"),
        P(("gr", "fs")),
    )
    return jax.shard_map(
        functools.partial(body, mesh.shape["gr"], mesh.shape["fs"], mesh.shape["tp"]),
        mesh=mesh,
        in_specs=placed,
        out_specs=(P(None, ("gr", "tp")), P(None, ("gr", "tp")), P(("gr", "fs", "tp"), None)),
        check_vma=False,
    )
```

```python
import functools

import jax
import jax.numpy as jnp
from jax import lax
from jax.experimental import pallas as pl
from jax.experimental.pallas import tpu as pltpu
from jax.sharding import PartitionSpec as P

MESH = pl.DeviceIdType.MESH
CHUNK = 32
TILE = 256
SPLIT = 4


def pair_share(count, width):
    share = []
    for quarters in (count * 5 // 8, count * 6 // 8):
        share.append((quarters // 4, quarters % 4 * (width // 4)))
    return share


def kernel(G, F, T, tok_in, gain_in, up_in, down_in, up_full, down_full, part,
           wide, narrow, raw, nrm, hid, stage,
           recv, dup, cross, cross_down, sendl, sendr, sendy, send0, tok_recv, tok_send,
           part_recv, part_send, local_sem, load_sem):
    gr, f, tp = lax.axis_index("gr"), lax.axis_index("fs"), lax.axis_index("tp")
    full = (up_full, down_full)
    A = F // 2
    a, y = f // 2, f % 2
    mate = a * 2 + 1 - y
    R = up_in.shape[0]
    D, W = up_full.shape
    tok = tok_in.shape[0]
    CH = min(CHUNK, R)
    C = R // CH
    NQ = G * C
    share = pair_share(NQ, W)
    K = G * T
    k = gr * T + tp
    weights = (up_in, down_in)

    def at_k(kk):
        return (kk // T, f, kk % T)

    def load(m, c):
        rows = pl.ds(c * CH, CH)
        return pltpu.make_async_copy(weights[m].at[rows], wide.at[m, rows], load_sem.at[m, c])

    for c in range(C):
        load(0, c).start()

    barrier = pltpu.get_barrier_semaphore()

    @pl.when(a > 0)
    def _():
        pl.semaphore_signal(barrier, inc=1, device_id=(gr, f - 2, tp), device_id_type=MESH)

    @pl.when(a < A - 1)
    def _():
        pl.semaphore_signal(barrier, inc=1, device_id=(gr, f + 2, tp), device_id_type=MESH)
    pl.semaphore_signal(barrier, inc=1, device_id=(gr, mate, tp), device_id_type=MESH)
    for d in range(1, K):
        pl.semaphore_signal(barrier, inc=1, device_id=at_k((k + d) % K), device_id_type=MESH)

    token_load = pltpu.make_async_copy(tok_in, raw, local_sem.at[0])
    for c in range(C):
        load(1, c).start()
    token_load.start()

    def rows_of(origin, g, c):
        return pl.ds(pl.multiple_of(g * (F * R) + origin * R + c * CH, CH), CH)

    home = k // G == tp

    def cast(m, c):
        rows = pl.ds(c * CH, CH)
        load(m, c).wait()
        value = wide[m, rows, :]
        if m == 0:
            value = value * column[c * CH:(c + 1) * CH]
        value = value.astype(jnp.bfloat16)
        narrow[m, rows, :] = value
        for b in range(G):
            @pl.when(tp * G + b == k)
            def _():
                full[m][rows_of(f, gr, c), :] = value[:, b * W:(b + 1) * W]

    def hand(m, b, c):
        kk = tp * G + b
        q = ((gr - kk // T + G) % G) * C + c

        @pl.when(kk != k)
        def _():
            copy = pltpu.make_async_remote_copy(
                src_ref=narrow.at[m, pl.ds(c * CH, CH), pl.ds(b * W, W)],
                dst_ref=full[m].at[rows_of(f, gr, c)],
                send_sem=send0.at[0], recv_sem=recv.at[m, a, q],
                device_id=at_k(kk), device_id_type=MESH)
            copy.start()

    mine = pl.ds(pl.multiple_of(k * tok, 16), tok)

    def tokens():
        for d in range(1, K):
            pltpu.make_async_remote_copy(
                src_ref=nrm.at[mine], dst_ref=nrm.at[mine],
                send_sem=tok_send.at[0], recv_sem=tok_recv.at[0],
                device_id=at_k((k + d) % K), device_id_type=MESH).start()

    def normalize(i, carry):
        values = raw[pl.ds(pl.multiple_of(i * 16, 16), 16), :].astype(jnp.float32)
        center = jnp.mean(values, axis=-1, keepdims=True)
        moved = values - center
        spread = jnp.mean(jnp.square(moved), axis=-1, keepdims=True)
        nrm[pl.ds(pl.multiple_of(k * tok + i * 16, 16), 16), :] = (
            moved * lax.rsqrt(spread + 1e-05)).astype(jnp.bfloat16)
        return carry

    rowed = lax.broadcasted_iota(jnp.int32, (R, R), 0) == lax.broadcasted_iota(jnp.int32, (R, R), 1)
    column = jnp.sum(jnp.where(rowed, gain_in[...], 0.0), axis=1, keepdims=True)

    def chunk(m, origin, q, columns):
        rows = rows_of(origin, (gr + q // C) % G, q % C)
        return full[m].at[rows, pl.ds(columns[0], columns[1] - columns[0])]

    def landing(m, origin_a, side, q):
        if side == "line":
            return recv.at[m, origin_a, q]
        if side == "pair":
            return dup.at[m, origin_a, q]
        return cross.at[0] if m == 0 else cross_down.at[origin_a, q // C]

    whole = (0, W)

    def send(m, origin, q, sem, side, target, columns=whole):
        ref = chunk(m, origin, q, columns)
        pltpu.make_async_remote_copy(
            src_ref=ref, dst_ref=ref, send_sem=sem.at[0], recv_sem=landing(m, origin // 2, side, q),
            device_id=(gr, target, tp), device_id_type=MESH).start()

    def await_rows(ref, count, sem):
        if count > 0:
            rows = ref.at[pl.ds(0, count)]
            pltpu.make_async_copy(rows, rows, sem).wait()

    def arrived(m, origin, q, side="line", columns=whole):
        ref = chunk(m, origin, q, columns)
        pltpu.make_async_copy(ref, ref, landing(m, origin // 2, side, q)).wait()

    def left(m, origin, q, side="line", columns=whole):
        @pl.when(a > 0)
        def _():
            send(m, origin, q, sendl, side, f - 2, columns)

    def right(m, origin, q, side="line", columns=whole):
        @pl.when(a < A - 1)
        def _():
            send(m, origin, q, sendr, side, f + 2, columns)

    def loop(low, high, step):
        def go(i, carry):
            step(i)
            return carry
        if high > low:
            lax.fori_loop(low, high, go, 0)

    def over_line(m):
        pf, shared = share[m]
        first = pf + (shared > 0)
        return ([(0, pf, ())] if pf else []) + ([(pf, first, (shared, W))] if shared else []), (first, C, whole)

    def over_pair(m):
        pf, shared = share[m]
        return ([(0, pf, whole)] if pf else []) + ([(pf, pf + 1, (0, shared))] if shared else [])

    def across(m, origin, q, columns):
        if columns:
            send(m, origin, q, sendy, "cross", mate, columns)

    def own_chunk(m, q, columns):
        left(m, f, q)
        right(m, f, q)
        if not columns:
            send(m, f, q, sendy, "pair", mate)
        elif columns[0] > 0:
            send(m, f, q, sendy, "pair", mate, (0, columns[0]))
        across(m, f, q, columns)

    def own(m):
        def near(columns):
            def step(q):
                if m == 0:
                    @pl.when(jnp.logical_not(home))
                    def _():
                        arrived(m, f, q)
                        own_chunk(m, q, columns)
                else:
                    @pl.when(jnp.logical_not(home))
                    def _():
                        arrived(m, f, q)
                    own_chunk(m, q, columns)
            return step

        def far(q):
            arrived(m, f, q)
            own_chunk(m, q, whole)

        shared, rest = over_line(m)
        for low, high, columns in shared:
            loop(low, high, near(columns))
        if m == 0:
            loop(rest[0], rest[1], near(whole))
            loop(C, NQ, far)
        else:
            loop(C, NQ, far)
            loop(rest[0], rest[1], near(whole))

    def mated(m):
        for low, high, columns in over_pair(m):
            def step(q):
                arrived(m, mate, q, "pair", columns)
                left(m, mate, q, "pair", columns)
                right(m, mate, q, "pair", columns)
            loop(low, high, step)

    def line(m, s, between=None, eager=None):
        below, above = a - 1 - s, a + 1 + s

        def both(side, columns):
            sent = columns if side == "pair" else whole

            def pass_on(origin, q, onward):
                arrived(m, origin, q, side, sent)
                onward(m, origin, q, side, sent)
                if side == "line":
                    across(m, origin, q, columns)

            def step(q):
                mine_y = y if side == "line" else 1 - y

                @pl.when(below >= 0)
                def _():
                    pass_on(below * 2 + mine_y, q, right)

                @pl.when(above < A)
                def _():
                    pass_on(above * 2 + mine_y, q, left)
            return step

        shared, rest = over_line(m)
        for low, high, columns in shared:
            loop(low, high, both("line", columns))
        if m == 0:
            loop(rest[0], rest[1], both("line", whole))
            loop(C, NQ, both("line", whole))
        else:
            loop(C, NQ, both("line", whole))
            if between is not None:
                between()
            loop(rest[0], rest[1], both("line", whole))
        if eager is not None:
            eager()
        for low, high, columns in over_pair(m):
            loop(low, high, both("pair", columns))

    def pair_rows(m):
        pf, shared = share[m]
        return pf * CH + CH * shared // W

    def settle_down(origin_a, gi):
        @pl.when(gi == 0)
        def _():
            await_rows(down_full, C * CH - pair_rows(1), cross_down.at[origin_a, 0])

        @pl.when(gi > 0)
        def _():
            await_rows(down_full, C * CH, cross_down.at[origin_a, gi])

    for c in range(C):
        cast(0, c)
        if c == 0:
            pl.semaphore_wait(barrier, K + (a > 0).astype(jnp.int32) + (a < A - 1).astype(jnp.int32))

        @pl.when(home)
        def _():
            pf, shared = share[0]
            own_chunk(0, c, () if c < pf else (shared if c == pf else 0, W))
        for b in range(G):
            hand(0, b, c)

    own(0)
    token_load.wait()
    lax.fori_loop(0, tok // 16, normalize, 0)
    for c in range(C):
        cast(1, c)
        for b in range(G):
            hand(1, b, c)
    tokens()
    mated(0)
    loop(0, A - 2, lambda s: line(0, s))
    own(1)
    line(0, A - 2)
    mated(1)
    line(1, 0)

    await_rows(up_full, A * (NQ * CH - pair_rows(0)), cross.at[0])
    await_rows(nrm, (K - 1) * tok, tok_recv.at[0])

    tile = min(TILE, W)

    def lift(j):
        columns = pl.ds(pl.multiple_of(j * tile, tile), tile)
        lifted = jnp.maximum(jnp.dot(nrm[...], up_full[:, columns], preferred_element_type=jnp.float32), 0.0)
        hid[:, columns] = (lifted * lifted).astype(jnp.bfloat16)
    loop(0, W // tile, lift)

    halves = 2 if R % 128 == 0 else 1

    def part_copy(d, block, columns):
        target = (k + d) % K
        return pltpu.make_async_remote_copy(
            src_ref=stage.at[block, pl.ds(pl.multiple_of(target * tok, 16), tok), columns],
            dst_ref=part.at[d - 1, block, :, columns],
            send_sem=part_send.at[0], recv_sem=part_recv.at[0],
            device_id=at_k(target), device_id_type=MESH)

    def multiply(block, rows, columns):
        value = lax.dot_general(hid[...], down_full[rows, :], (((1,), (1,)), ((), ())),
                                preferred_element_type=jnp.float32)
        stage[block, :, columns] = value.astype(jnp.bfloat16)
        part[K - 1, block, :, columns] = stage[block, mine, columns]
        for d in range(1, K):
            part_copy(d, block, columns).start()

    def lower(origin_a, gi):
        settle_down(origin_a, gi)
        g = (gr + gi) % G
        rows = pl.ds(pl.multiple_of(g * (F * R) + origin_a * (2 * R), 2 * R), 2 * R)
        multiply(origin_a * G + g, rows, pl.ds(0, 2 * R))

    def lower_half(origin_a, side):
        rows = pl.ds(pl.multiple_of(gr * (F * R) + (origin_a * 2 + side) * R, R), R)
        multiply(origin_a * G + gr, rows, pl.ds(pl.multiple_of(side * R, R), R))

    def ends(step):
        @pl.when(a - 1 - (A - 2) >= 0)
        def _():
            step(a - 1 - (A - 2))

        @pl.when(a + 1 + (A - 2) < A)
        def _():
            step(a + 1 + (A - 2))

    def early():
        lower_ring(A - 2, 0, G - 1)
        if halves == 2:
            ends(lambda origin_a: lower_half(origin_a, y))

    def late():
        if halves == 2:
            def step(origin_a):
                settle_down(origin_a, 0)
                lower_half(origin_a, 1 - y)
            ends(step)
        else:
            lower_ring(A - 2, G - 1, G)

    def lower_ring(s, low=0, high=G):
        @pl.when(a - 1 - s >= 0)
        def _():
            loop(low, high, lambda i: lower(a - 1 - s, G - 1 - i))

        @pl.when(a + 1 + s < A)
        def _():
            loop(low, high, lambda i: lower(a + 1 + s, G - 1 - i))

    loop(0, G, lambda i: lower(a, G - 1 - i))
    loop(1, A - 2, lambda s: line(1, s, between=lambda: lower_ring(s - 1)))
    line(1, A - 2, between=lambda: lower_ring(A - 3), eager=early)
    late()

    await_rows(part, K - 1, part_recv.at[0])
    await_rows(part, K - 1, part_send.at[0])
    await_rows(nrm, (K - 1) * tok, tok_send.at[0])
    pairs = pair_rows(0) + pair_rows(1)
    await_rows(up_full, 2 * NQ * CH, sendy.at[0])
    for _ in range(A - 1):
        await_rows(up_full, 2 * NQ * CH - pairs, sendy.at[0])

    def drain(sem, rows):
        def step(i, carry):
            await_rows(up_full, rows, sem.at[0])
            return carry
        return step
    lax.fori_loop(0, jnp.where(a > 0, A - a, 0), drain(sendl, 2 * NQ * CH + pairs), 0)
    lax.fori_loop(0, jnp.where(a < A - 1, a + 1, 0), drain(sendr, 2 * NQ * CH + pairs), 0)
    lax.fori_loop(0, jnp.where(home, G - 1, G), drain(send0, 2 * R), 0)


def finish(G, F, up_held, down_held, parts, up_out, down_out, out_ref, summed, sems, out_sem):
    def out(m, i):
        source, target = ((up_held, up_out), (down_held, down_out))[m]
        size = source.shape[0] // SPLIT
        rows = pl.ds(i * size, size)
        return pltpu.make_async_copy(source.at[rows], target.at[rows], sems.at[m, i])

    for m in range(2):
        for i in range(SPLIT):
            out(m, i).start()
    K, blocks, _, wide = parts.shape
    D = out_ref.shape[1]
    for block in range(blocks):
        total = parts[0, block].astype(jnp.float32)
        for i in range(1, K):
            total += parts[i, block].astype(jnp.float32)
        begin = (block % G) * (D // G) + (block // G) * wide
        summed[:, begin:begin + wide] = total.astype(jnp.bfloat16)
    tokens_out = pltpu.make_async_copy(summed, out_ref, out_sem.at[0])
    tokens_out.start()
    for m in range(2):
        for i in range(SPLIT):
            out(m, i).wait()
    tokens_out.wait()


def body(G, F, T, prompt_tokens, up_master, down_master, norm_gain):
    R, width = up_master.shape
    tok = prompt_tokens.shape[0]
    D, W = R * G * F, width // G
    A, K = F // 2, G * T
    C = R // min(CHUNK, R)
    NQ = G * C
    pairs = max(1, max(pf + (shared > 0) for pf, shared in pair_share(NQ, W)))
    bf16 = jnp.bfloat16
    any_space = pl.BlockSpec(memory_space=pl.ANY)
    vmem_space = pl.BlockSpec(memory_space=pltpu.VMEM)
    dma = pltpu.SemaphoreType.DMA
    up_held, down_held, parts = pl.pallas_call(
        functools.partial(kernel, G, F, T),
        name="handoff",
        out_shape=(
            pltpu.MemorySpace.VMEM((D, W), bf16),
            pltpu.MemorySpace.VMEM((D, W), bf16),
            pltpu.MemorySpace.VMEM((K, A * G, tok, 2 * R), bf16),
        ),
        in_specs=[any_space, vmem_space, any_space, any_space],
        out_specs=(vmem_space,) * 3,
        scratch_shapes=[
            pltpu.VMEM((2, R, width), jnp.float32),
            pltpu.VMEM((2, R, width), bf16),
            pltpu.VMEM((tok, D), bf16),
            pltpu.VMEM((K * tok, D), bf16),
            pltpu.VMEM((K * tok, W), bf16),
            pltpu.VMEM((A * G, K * tok, 2 * R), bf16),
            dma((2, A, NQ)), dma((2, A, pairs)), dma((1,)), dma((A, G)),
            dma((1,)), dma((1,)), dma((1,)), dma((1,)), dma((1,)), dma((1,)),
            dma((1,)), dma((1,)), dma((1,)), dma((2, C)),
        ],
        compiler_params=pltpu.CompilerParams(
            collective_id=0, has_side_effects=True, vmem_limit_bytes=41 * 1024 * 1024),
    )(prompt_tokens, norm_gain.reshape(1, R), up_master, down_master)
    return pl.pallas_call(
        functools.partial(finish, G, F),
        name="finish",
        out_shape=(
            jax.ShapeDtypeStruct((D, W), bf16),
            jax.ShapeDtypeStruct((D, W), bf16),
            jax.ShapeDtypeStruct((tok, D), bf16),
        ),
        in_specs=[vmem_space] * 3,
        out_specs=(any_space, any_space, any_space),
        scratch_shapes=[pltpu.VMEM((tok, D), bf16), dma((2, SPLIT)), dma((1,))],
        compiler_params=pltpu.CompilerParams(vmem_limit_bytes=16 * 1024 * 1024),
    )(up_held, down_held, parts)


def solution(mesh):
    placed = (
        P(("gr", "fs", "tp"), None),
        P(("gr", "fs"), "tp"),
        P(("gr", "fs"), "tp"),
        P(("gr", "fs")),
    )
    return jax.shard_map(
        functools.partial(body, mesh.shape["gr"], mesh.shape["fs"], mesh.shape["tp"]),
        mesh=mesh,
        in_specs=placed,
        out_specs=(P(None, ("gr", "tp")), P(None, ("gr", "tp")), P(("gr", "fs", "tp"), None)),
        check_vma=False,
    )
```

```python
import functools

import jax
import jax.numpy as jnp
from jax import lax
from jax.experimental import pallas as pl
from jax.experimental.pallas import tpu as pltpu
from jax.sharding import PartitionSpec as P

MESH = pl.DeviceIdType.MESH
CHUNK = 32
TILE = 256
SPLIT = 4


def pair_share(count, width):
    share = []
    for quarters in (count * 5 // 8, count * 6 // 8):
        share.append((quarters // 4, quarters % 4 * (width // 4)))
    return share


def kernel(G, F, T, tok_in, gain_in, up_in, down_in, up_full, down_full, part,
           wide, narrow, raw, nrm, hid, stage,
           recv, dup, cross, cross_down, sendl, sendr, sendy, send0, tok_recv, tok_send,
           part_recv, part_send, local_sem, load_sem):
    gr, f, tp = lax.axis_index("gr"), lax.axis_index("fs"), lax.axis_index("tp")
    full = (up_full, down_full)
    A = F // 2
    a, y = f // 2, f % 2
    mate = a * 2 + 1 - y
    R = up_in.shape[0]
    D, W = up_full.shape
    tok = tok_in.shape[0]
    CH = min(CHUNK, R)
    C = R // CH
    NQ = G * C
    share = pair_share(NQ, W)
    K = G * T
    k = gr * T + tp
    weights = (up_in, down_in)

    def at_k(kk):
        return (kk // T, f, kk % T)

    def load(m, c):
        rows = pl.ds(c * CH, CH)
        return pltpu.make_async_copy(weights[m].at[rows], wide.at[m, rows], load_sem.at[m, c])

    for c in range(C):
        load(0, c).start()

    barrier = pltpu.get_barrier_semaphore()

    @pl.when(a > 0)
    def _():
        pl.semaphore_signal(barrier, inc=1, device_id=(gr, f - 2, tp), device_id_type=MESH)

    @pl.when(a < A - 1)
    def _():
        pl.semaphore_signal(barrier, inc=1, device_id=(gr, f + 2, tp), device_id_type=MESH)
    pl.semaphore_signal(barrier, inc=1, device_id=(gr, mate, tp), device_id_type=MESH)
    for d in range(1, K):
        pl.semaphore_signal(barrier, inc=1, device_id=at_k((k + d) % K), device_id_type=MESH)

    token_load = pltpu.make_async_copy(tok_in, raw, local_sem.at[0])
    for c in range(C):
        load(1, c).start()
    token_load.start()

    def rows_of(origin, g, c):
        return pl.ds(pl.multiple_of(g * (F * R) + origin * R + c * CH, CH), CH)

    home = k // G == tp

    def cast(m, c):
        rows = pl.ds(c * CH, CH)
        load(m, c).wait()
        value = wide[m, rows, :]
        if m == 0:
            value = value * column[c * CH:(c + 1) * CH]
        value = value.astype(jnp.bfloat16)
        narrow[m, rows, :] = value
        for b in range(G):
            @pl.when(tp * G + b == k)
            def _():
                full[m][rows_of(f, gr, c), :] = value[:, b * W:(b + 1) * W]

    def hand(m, b, c):
        kk = tp * G + b
        q = ((gr - kk // T + G) % G) * C + c

        @pl.when(kk != k)
        def _():
            copy = pltpu.make_async_remote_copy(
                src_ref=narrow.at[m, pl.ds(c * CH, CH), pl.ds(b * W, W)],
                dst_ref=full[m].at[rows_of(f, gr, c)],
                send_sem=send0.at[0], recv_sem=recv.at[m, a, q],
                device_id=at_k(kk), device_id_type=MESH)
            copy.start()

    mine = pl.ds(pl.multiple_of(k * tok, 16), tok)

    def tokens():
        for d in range(1, K):
            pltpu.make_async_remote_copy(
                src_ref=nrm.at[mine], dst_ref=nrm.at[mine],
                send_sem=tok_send.at[0], recv_sem=tok_recv.at[0],
                device_id=at_k((k + d) % K), device_id_type=MESH).start()

    def normalize(i, carry):
        values = raw[pl.ds(pl.multiple_of(i * 16, 16), 16), :].astype(jnp.float32)
        center = jnp.mean(values, axis=-1, keepdims=True)
        moved = values - center
        spread = jnp.mean(jnp.square(moved), axis=-1, keepdims=True)
        nrm[pl.ds(pl.multiple_of(k * tok + i * 16, 16), 16), :] = (
            moved * lax.rsqrt(spread + 1e-05)).astype(jnp.bfloat16)
        return carry

    rowed = lax.broadcasted_iota(jnp.int32, (R, R), 0) == lax.broadcasted_iota(jnp.int32, (R, R), 1)
    column = jnp.sum(jnp.where(rowed, gain_in[...], 0.0), axis=1, keepdims=True)

    def chunk(m, origin, q, columns):
        rows = rows_of(origin, (gr + q // C) % G, q % C)
        return full[m].at[rows, pl.ds(columns[0], columns[1] - columns[0])]

    def landing(m, origin_a, side, q):
        if side == "line":
            return recv.at[m, origin_a, q]
        if side == "pair":
            return dup.at[m, origin_a, q]
        return cross.at[0] if m == 0 else cross_down.at[origin_a, q // C]

    whole = (0, W)

    def send(m, origin, q, sem, side, target, columns=whole):
        ref = chunk(m, origin, q, columns)
        pltpu.make_async_remote_copy(
            src_ref=ref, dst_ref=ref, send_sem=sem.at[0], recv_sem=landing(m, origin // 2, side, q),
            device_id=(gr, target, tp), device_id_type=MESH).start()

    def await_rows(ref, count, sem):
        if count > 0:
            rows = ref.at[pl.ds(0, count)]
            pltpu.make_async_copy(rows, rows, sem).wait()

    def arrived(m, origin, q, side="line", columns=whole):
        ref = chunk(m, origin, q, columns)
        pltpu.make_async_copy(ref, ref, landing(m, origin // 2, side, q)).wait()

    def left(m, origin, q, side="line", columns=whole):
        @pl.when(a > 0)
        def _():
            send(m, origin, q, sendl, side, f - 2, columns)

    def right(m, origin, q, side="line", columns=whole):
        @pl.when(a < A - 1)
        def _():
            send(m, origin, q, sendr, side, f + 2, columns)

    def loop(low, high, step):
        def go(i, carry):
            step(i)
            return carry
        if high > low:
            lax.fori_loop(low, high, go, 0)

    def over_line(m):
        pf, shared = share[m]
        first = pf + (shared > 0)
        return ([(0, pf, ())] if pf else []) + ([(pf, first, (shared, W))] if shared else []), (first, C, whole)

    def over_pair(m):
        pf, shared = share[m]
        return ([(0, pf, whole)] if pf else []) + ([(pf, pf + 1, (0, shared))] if shared else [])

    def across(m, origin, q, columns):
        if columns:
            send(m, origin, q, sendy, "cross", mate, columns)

    def own_chunk(m, q, columns, pair=True):
        left(m, f, q)
        right(m, f, q)
        if pair and columns[:1] != (0,):
            send(m, f, q, sendy, "pair", mate, (0, columns[0]) if columns else whole)
        across(m, f, q, columns)

    def own(m):
        def near(columns):
            def step(q):
                @pl.when(jnp.logical_not(home))
                def _():
                    arrived(m, f, q)
                    if m == 0:
                        own_chunk(m, q, columns)
                if m > 0:
                    own_chunk(m, q, columns, False)
            return step

        def far(q):
            arrived(m, f, q)
            own_chunk(m, q, whole)

        shared, rest = over_line(m)
        if m == 0:
            for low, high, columns in shared:
                loop(low, high, near(columns))
            loop(rest[0], rest[1], near(whole))
            loop(C, NQ, far)
        else:
            for low, high, columns in over_pair(m):
                def step(q):
                    @pl.when(jnp.logical_not(home))
                    def _():
                        arrived(m, f, q)
                    send(m, f, q, sendy, "pair", mate, columns)
                loop(low, high, step)

            loop(C, NQ, far)

            def step(columns):
                def go(q):
                    own_chunk(m, q, columns, False)
                return go
            for low, high, columns in shared:
                if columns:
                    loop(low, high, step(columns))
            loop(rest[0], rest[1], near(whole))
            for low, high, columns in shared:
                if not columns:
                    loop(low, high, step(columns))

    def mated(m):
        for low, high, columns in over_pair(m):
            def step(q):
                arrived(m, mate, q, "pair", columns)
                left(m, mate, q, "pair", columns)
                right(m, mate, q, "pair", columns)
            loop(low, high, step)

    def line(m, s, between=None, eager=None):
        below, above = a - 1 - s, a + 1 + s

        def both(side, columns):
            sent = columns if side == "pair" else whole

            def pass_on(origin, q, onward):
                arrived(m, origin, q, side, sent)
                onward(m, origin, q, side, sent)
                if side == "line":
                    across(m, origin, q, columns)

            def step(q):
                mine_y = y if side == "line" else 1 - y

                @pl.when(below >= 0)
                def _():
                    pass_on(below * 2 + mine_y, q, right)

                @pl.when(above < A)
                def _():
                    pass_on(above * 2 + mine_y, q, left)
            return step

        shared, rest = over_line(m)
        if m == 0:
            for low, high, columns in shared:
                loop(low, high, both("line", columns))
            loop(rest[0], rest[1], both("line", whole))
            loop(C, NQ, both("line", whole))
        else:
            loop(C, NQ, both("line", whole))
            if between is not None:
                between()
            for low, high, columns in shared:
                if columns:
                    loop(low, high, both("line", columns))
            loop(rest[0], rest[1], both("line", whole))
            for low, high, columns in shared:
                if not columns:
                    loop(low, high, both("line", columns))
        if eager is not None:
            eager()
        for low, high, columns in over_pair(m):
            loop(low, high, both("pair", columns))

    def pair_rows(m):
        pf, shared = share[m]
        return pf * CH + CH * shared // W

    def settle_down(origin_a, gi):
        @pl.when(gi == 0)
        def _():
            await_rows(down_full, C * CH - pair_rows(1), cross_down.at[origin_a, 0])

        @pl.when(gi > 0)
        def _():
            await_rows(down_full, C * CH, cross_down.at[origin_a, gi])

    for c in range(C):
        cast(0, c)
        if c == 0:
            pl.semaphore_wait(barrier, K + (a > 0).astype(jnp.int32) + (a < A - 1).astype(jnp.int32))

        @pl.when(home)
        def _():
            pf, shared = share[0]
            own_chunk(0, c, () if c < pf else (shared if c == pf else 0, W))
        for b in range(G):
            hand(0, b, c)

    own(0)
    token_load.wait()
    lax.fori_loop(0, tok // 16, normalize, 0)
    for c in range(C):
        cast(1, c)
        for b in range(G):
            hand(1, b, c)
    tokens()
    mated(0)
    loop(0, A - 2, lambda s: line(0, s))
    own(1)
    line(0, A - 2)
    mated(1)
    line(1, 0)

    await_rows(up_full, A * (NQ * CH - pair_rows(0)), cross.at[0])
    await_rows(nrm, (K - 1) * tok, tok_recv.at[0])

    tile = min(TILE, W)

    def lift(j):
        columns = pl.ds(pl.multiple_of(j * tile, tile), tile)
        lifted = jnp.maximum(jnp.dot(nrm[...], up_full[:, columns], preferred_element_type=jnp.float32), 0.0)
        hid[:, columns] = (lifted * lifted).astype(jnp.bfloat16)
    loop(0, W // tile, lift)

    halves = 2 if R % 128 == 0 else 1

    def part_copy(d, block, columns):
        target = (k + d) % K
        return pltpu.make_async_remote_copy(
            src_ref=stage.at[block, pl.ds(pl.multiple_of(target * tok, 16), tok), columns],
            dst_ref=part.at[d - 1, block, :, columns],
            send_sem=part_send.at[0], recv_sem=part_recv.at[0],
            device_id=at_k(target), device_id_type=MESH)

    def multiply(block, rows, columns):
        value = lax.dot_general(hid[...], down_full[rows, :], (((1,), (1,)), ((), ())),
                                preferred_element_type=jnp.float32)
        stage[block, :, columns] = value.astype(jnp.bfloat16)
        part[K - 1, block, :, columns] = stage[block, mine, columns]
        for d in range(1, K):
            part_copy(d, block, columns).start()

    def lower(origin_a, gi):
        settle_down(origin_a, gi)
        g = (gr + gi) % G
        rows = pl.ds(pl.multiple_of(g * (F * R) + origin_a * (2 * R), 2 * R), 2 * R)
        multiply(origin_a * G + g, rows, pl.ds(0, 2 * R))

    def lower_half(origin_a, side):
        rows = pl.ds(pl.multiple_of(gr * (F * R) + (origin_a * 2 + side) * R, R), R)
        multiply(origin_a * G + gr, rows, pl.ds(pl.multiple_of(side * R, R), R))

    def ends(step):
        @pl.when(a - 1 - (A - 2) >= 0)
        def _():
            step(a - 1 - (A - 2))

        @pl.when(a + 1 + (A - 2) < A)
        def _():
            step(a + 1 + (A - 2))

    def early():
        lower_ring(A - 2, 0, G - 1)
        if halves == 2:
            ends(lambda origin_a: lower_half(origin_a, y))

    def late():
        if halves == 2:
            def step(origin_a):
                settle_down(origin_a, 0)
                lower_half(origin_a, 1 - y)
            ends(step)
        else:
            lower_ring(A - 2, G - 1, G)

    def lower_ring(s, low=0, high=G):
        @pl.when(a - 1 - s >= 0)
        def _():
            loop(low, high, lambda i: lower(a - 1 - s, G - 1 - i))

        @pl.when(a + 1 + s < A)
        def _():
            loop(low, high, lambda i: lower(a + 1 + s, G - 1 - i))

    loop(0, G, lambda i: lower(a, G - 1 - i))
    loop(1, A - 2, lambda s: line(1, s, between=lambda: lower_ring(s - 1)))
    line(1, A - 2, between=lambda: lower_ring(A - 3), eager=early)
    late()

    await_rows(part, K - 1, part_recv.at[0])
    await_rows(part, K - 1, part_send.at[0])
    await_rows(nrm, (K - 1) * tok, tok_send.at[0])
    pairs = pair_rows(0) + pair_rows(1)
    await_rows(up_full, 2 * NQ * CH, sendy.at[0])
    for _ in range(A - 1):
        await_rows(up_full, 2 * NQ * CH - pairs, sendy.at[0])

    def drain(sem, rows):
        def step(i, carry):
            await_rows(up_full, rows, sem.at[0])
            return carry
        return step
    lax.fori_loop(0, jnp.where(a > 0, A - a, 0), drain(sendl, 2 * NQ * CH + pairs), 0)
    lax.fori_loop(0, jnp.where(a < A - 1, a + 1, 0), drain(sendr, 2 * NQ * CH + pairs), 0)
    lax.fori_loop(0, jnp.where(home, G - 1, G), drain(send0, 2 * R), 0)


def finish(G, F, up_held, down_held, parts, up_out, down_out, out_ref, summed, sems, out_sem):
    def out(m, i):
        source, target = ((up_held, up_out), (down_held, down_out))[m]
        size = source.shape[0] // SPLIT
        rows = pl.ds(i * size, size)
        return pltpu.make_async_copy(source.at[rows], target.at[rows], sems.at[m, i])

    for m in range(2):
        for i in range(SPLIT):
            out(m, i).start()
    K, blocks, _, wide = parts.shape
    D = out_ref.shape[1]
    for block in range(blocks):
        total = parts[0, block].astype(jnp.float32)
        for i in range(1, K):
            total += parts[i, block].astype(jnp.float32)
        begin = (block % G) * (D // G) + (block // G) * wide
        summed[:, begin:begin + wide] = total.astype(jnp.bfloat16)
    tokens_out = pltpu.make_async_copy(summed, out_ref, out_sem.at[0])
    tokens_out.start()
    for m in range(2):
        for i in range(SPLIT):
            out(m, i).wait()
    tokens_out.wait()


def body(G, F, T, prompt_tokens, up_master, down_master, norm_gain):
    R, width = up_master.shape
    tok = prompt_tokens.shape[0]
    D, W = R * G * F, width // G
    A, K = F // 2, G * T
    C = R // min(CHUNK, R)
    NQ = G * C
    pairs = max(1, max(pf + (shared > 0) for pf, shared in pair_share(NQ, W)))
    bf16 = jnp.bfloat16
    any_space = pl.BlockSpec(memory_space=pl.ANY)
    vmem_space = pl.BlockSpec(memory_space=pltpu.VMEM)
    dma = pltpu.SemaphoreType.DMA
    up_held, down_held, parts = pl.pallas_call(
        functools.partial(kernel, G, F, T),
        name="handoff",
        out_shape=(
            pltpu.MemorySpace.VMEM((D, W), bf16),
            pltpu.MemorySpace.VMEM((D, W), bf16),
            pltpu.MemorySpace.VMEM((K, A * G, tok, 2 * R), bf16),
        ),
        in_specs=[any_space, vmem_space, any_space, any_space],
        out_specs=(vmem_space,) * 3,
        scratch_shapes=[
            pltpu.VMEM((2, R, width), jnp.float32),
            pltpu.VMEM((2, R, width), bf16),
            pltpu.VMEM((tok, D), bf16),
            pltpu.VMEM((K * tok, D), bf16),
            pltpu.VMEM((K * tok, W), bf16),
            pltpu.VMEM((A * G, K * tok, 2 * R), bf16),
            dma((2, A, NQ)), dma((2, A, pairs)), dma((1,)), dma((A, G)),
            dma((1,)), dma((1,)), dma((1,)), dma((1,)), dma((1,)), dma((1,)),
            dma((1,)), dma((1,)), dma((1,)), dma((2, C)),
        ],
        compiler_params=pltpu.CompilerParams(
            collective_id=0, has_side_effects=True, vmem_limit_bytes=41 * 1024 * 1024),
    )(prompt_tokens, norm_gain.reshape(1, R), up_master, down_master)
    return pl.pallas_call(
        functools.partial(finish, G, F),
        name="finish",
        out_shape=(
            jax.ShapeDtypeStruct((D, W), bf16),
            jax.ShapeDtypeStruct((D, W), bf16),
            jax.ShapeDtypeStruct((tok, D), bf16),
        ),
        in_specs=[vmem_space] * 3,
        out_specs=(any_space, any_space, any_space),
        scratch_shapes=[pltpu.VMEM((tok, D), bf16), dma((2, SPLIT)), dma((1,))],
        compiler_params=pltpu.CompilerParams(vmem_limit_bytes=16 * 1024 * 1024),
    )(up_held, down_held, parts)


def solution(mesh):
    placed = (
        P(("gr", "fs", "tp"), None),
        P(("gr", "fs"), "tp"),
        P(("gr", "fs"), "tp"),
        P(("gr", "fs")),
    )
    return jax.shard_map(
        functools.partial(body, mesh.shape["gr"], mesh.shape["fs"], mesh.shape["tp"]),
        mesh=mesh,
        in_specs=placed,
        out_specs=(P(None, ("gr", "tp")), P(None, ("gr", "tp")), P(("gr", "fs", "tp"), None)),
        check_vma=False,
    )
```

```python
import functools

import jax
import jax.numpy as jnp
from jax import lax
from jax.experimental import pallas as pl
from jax.experimental.pallas import tpu as pltpu
from jax.sharding import PartitionSpec as P

MESH = pl.DeviceIdType.MESH
CHUNK = 32
TILE = 256
SPLIT = 4


def pair_share(count, width):
    share = []
    for quarters in (count * 5 // 8, count * 6 // 8):
        share.append((quarters // 4, quarters % 4 * (width // 4)))
    return share


def kernel(G, F, T, tok_in, gain_in, up_in, down_in, up_full, down_full, part,
           wide, narrow, raw, nrm, hid, stage,
           recv, dup, cross, cross_down, sendl, sendr, sendy, send0, tok_recv, tok_send,
           part_recv, part_send, local_sem, load_sem, ready):
    gr, f, tp = lax.axis_index("gr"), lax.axis_index("fs"), lax.axis_index("tp")
    full = (up_full, down_full)
    A = F // 2
    a, y = f // 2, f % 2
    mate = a * 2 + 1 - y
    R = up_in.shape[0]
    D, W = up_full.shape
    tok = tok_in.shape[0]
    CH = min(CHUNK, R)
    C = R // CH
    NQ = G * C
    share = pair_share(NQ, W)
    K = G * T
    k = gr * T + tp
    weights = (up_in, down_in)

    def at_k(kk):
        return (kk // T, f, kk % T)

    def load(m, c):
        rows = pl.ds(c * CH, CH)
        return pltpu.make_async_copy(weights[m].at[rows], wide.at[m, rows], load_sem.at[m, c])

    load(0, 0).start()
    barrier = pltpu.get_barrier_semaphore()

    @pl.when(a < A - 1)
    def _():
        pl.semaphore_signal(barrier, inc=1, device_id=(gr, f + 2, tp), device_id_type=MESH)

    @pl.when(y == 0)
    def _():
        pl.semaphore_signal(barrier, inc=1, device_id=(gr, mate, tp), device_id_type=MESH)

    for kk in range(1, K):
        @pl.when(kk > k)
        def _():
            pl.semaphore_signal(barrier, inc=1, device_id=at_k(kk), device_id_type=MESH)

    token_load = pltpu.make_async_copy(tok_in, raw, local_sem.at[0])
    for c in range(1, C):
        load(0, c).start()
    partners = (a > 0).astype(jnp.int32) + y + k

    @pl.when(partners > 0)
    def _():
        pl.semaphore_wait(barrier, partners)

    @pl.when(a > 0)
    def _():
        pl.semaphore_signal(ready.at[0], inc=1, device_id=(gr, f - 2, tp), device_id_type=MESH)

    @pl.when(y == 1)
    def _():
        pl.semaphore_signal(ready.at[1], inc=1, device_id=(gr, mate, tp), device_id_type=MESH)

    for kk in range(K - 1):
        @pl.when(kk < k)
        def _():
            pl.semaphore_signal(ready.at[2], inc=1, device_id=at_k(kk), device_id_type=MESH)

    def rows_of(origin, g, c):
        return pl.ds(pl.multiple_of(g * (F * R) + origin * R + c * CH, CH), CH)

    home = k // G == tp

    def cast(m, c):
        rows = pl.ds(c * CH, CH)
        load(m, c).wait()
        value = wide[m, rows, :]
        if m == 0:
            value = value * column[c * CH:(c + 1) * CH]
        value = value.astype(jnp.bfloat16)
        narrow[m, rows, :] = value
        for b in range(G):
            @pl.when(tp * G + b == k)
            def _():
                full[m][rows_of(f, gr, c), :] = value[:, b * W:(b + 1) * W]

    def hand(m, b, c):
        kk = tp * G + b
        q = ((gr - kk // T + G) % G) * C + c

        @pl.when(kk != k)
        def _():
            copy = pltpu.make_async_remote_copy(
                src_ref=narrow.at[m, pl.ds(c * CH, CH), pl.ds(b * W, W)],
                dst_ref=full[m].at[rows_of(f, gr, c)],
                send_sem=send0.at[0], recv_sem=recv.at[m, a, q],
                device_id=at_k(kk), device_id_type=MESH)
            copy.start()

    mine = pl.ds(pl.multiple_of(k * tok, 16), tok)

    def tokens():
        for d in range(1, K):
            pltpu.make_async_remote_copy(
                src_ref=nrm.at[mine], dst_ref=nrm.at[mine],
                send_sem=tok_send.at[0], recv_sem=tok_recv.at[0],
                device_id=at_k((k + d) % K), device_id_type=MESH).start()

    def normalize(i, carry):
        values = raw[pl.ds(pl.multiple_of(i * 16, 16), 16), :].astype(jnp.float32)
        center = jnp.mean(values, axis=-1, keepdims=True)
        moved = values - center
        spread = jnp.mean(jnp.square(moved), axis=-1, keepdims=True)
        nrm[pl.ds(pl.multiple_of(k * tok + i * 16, 16), 16), :] = (
            moved * lax.rsqrt(spread + 1e-05)).astype(jnp.bfloat16)
        return carry

    rowed = lax.broadcasted_iota(jnp.int32, (R, R), 0) == lax.broadcasted_iota(jnp.int32, (R, R), 1)
    column = jnp.sum(jnp.where(rowed, gain_in[...], 0.0), axis=1, keepdims=True)

    def chunk(m, origin, q, columns):
        rows = rows_of(origin, (gr + q // C) % G, q % C)
        return full[m].at[rows, pl.ds(columns[0], columns[1] - columns[0])]

    def landing(m, origin_a, side, q):
        if side == "line":
            return recv.at[m, origin_a, q]
        if side == "pair":
            return dup.at[m, origin_a, q]
        return cross.at[0] if m == 0 else cross_down.at[origin_a, q // C]

    whole = (0, W)

    def send(m, origin, q, sem, side, target, columns=whole):
        ref = chunk(m, origin, q, columns)
        pltpu.make_async_remote_copy(
            src_ref=ref, dst_ref=ref, send_sem=sem.at[0], recv_sem=landing(m, origin // 2, side, q),
            device_id=(gr, target, tp), device_id_type=MESH).start()

    def await_rows(ref, count, sem):
        if count > 0:
            rows = ref.at[pl.ds(0, count)]
            pltpu.make_async_copy(rows, rows, sem).wait()

    def arrived(m, origin, q, side="line", columns=whole):
        ref = chunk(m, origin, q, columns)
        pltpu.make_async_copy(ref, ref, landing(m, origin // 2, side, q)).wait()

    def left(m, origin, q, side="line", columns=whole):
        @pl.when(a > 0)
        def _():
            send(m, origin, q, sendl, side, f - 2, columns)

    def right(m, origin, q, side="line", columns=whole):
        @pl.when(a < A - 1)
        def _():
            send(m, origin, q, sendr, side, f + 2, columns)

    def loop(low, high, step):
        def go(i, carry):
            step(i)
            return carry
        if high > low:
            lax.fori_loop(low, high, go, 0)

    def over_line(m):
        pf, shared = share[m]
        first = pf + (shared > 0)
        return ([(0, pf, ())] if pf else []) + ([(pf, first, (shared, W))] if shared else []), (first, C, whole)

    def over_pair(m):
        pf, shared = share[m]
        return ([(0, pf, whole)] if pf else []) + ([(pf, pf + 1, (0, shared))] if shared else [])

    def across(m, origin, q, columns):
        if columns:
            send(m, origin, q, sendy, "cross", mate, columns)

    def own_chunk(m, q, columns, pair=True, down_line=True):
        if down_line:
            left(m, f, q)
        right(m, f, q)
        if pair and columns[:1] != (0,):
            send(m, f, q, sendy, "pair", mate, (0, columns[0]) if columns else whole)
        across(m, f, q, columns)

    def own(m):
        def near(columns):
            def step(q):
                @pl.when(jnp.logical_not(home))
                def _():
                    arrived(m, f, q)
                    if m == 0:
                        own_chunk(m, q, columns)
                if m > 0:
                    own_chunk(m, q, columns, False)
            return step

        def far(q):
            arrived(m, f, q)
            own_chunk(m, q, whole)

        shared, rest = over_line(m)
        if m == 0:
            for low, high, columns in shared:
                loop(low, high, near(columns))
            loop(rest[0], rest[1], near(whole))
            loop(C, NQ, far)
        else:
            for low, high, columns in over_pair(m):
                def step(q):
                    @pl.when(jnp.logical_not(home))
                    def _():
                        arrived(m, f, q)
                    send(m, f, q, sendy, "pair", mate, columns)
                loop(low, high, step)

            loop(C, NQ, far)

            def step(columns):
                def go(q):
                    own_chunk(m, q, columns, False)
                return go
            for low, high, columns in shared:
                if columns:
                    loop(low, high, step(columns))
            loop(rest[0], rest[1], near(whole))
            for low, high, columns in shared:
                if not columns:
                    loop(low, high, step(columns))

    def mated(m):
        for low, high, columns in over_pair(m):
            def step(q):
                arrived(m, mate, q, "pair", columns)
                left(m, mate, q, "pair", columns)
                right(m, mate, q, "pair", columns)
            loop(low, high, step)

    def line(m, s, between=None, eager=None, closing=None):
        below, above = a - 1 - s, a + 1 + s

        def both(side, columns):
            sent = columns if side == "pair" else whole

            def pass_on(origin, q, onward):
                arrived(m, origin, q, side, sent)
                onward(m, origin, q, side, sent)
                if side == "line":
                    across(m, origin, q, columns)

            def step(q):
                mine_y = y if side == "line" else 1 - y

                @pl.when(below >= 0)
                def _():
                    pass_on(below * 2 + mine_y, q, right)

                @pl.when(above < A)
                def _():
                    pass_on(above * 2 + mine_y, q, left)
            return step

        shared, rest = over_line(m)
        if m == 0:
            for low, high, columns in shared:
                loop(low, high, both("line", columns))
            loop(rest[0], rest[1], both("line", whole))
            loop(C, NQ, both("line", whole))
        else:
            loop(C, NQ, both("line", whole))
            if between is not None:
                between()
            for low, high, columns in shared:
                if columns:
                    loop(low, high, both("line", columns))
            loop(rest[0], rest[1], both("line", whole))
            if eager is not None:
                eager()
            for low, high, columns in shared:
                if not columns:
                    loop(low, high, both("line", columns))
        if closing is not None:
            closing()
        for low, high, columns in over_pair(m):
            loop(low, high, both("pair", columns))

    def pair_rows(m):
        pf, shared = share[m]
        return pf * CH + CH * shared // W

    def settle_down(origin_a, gi):
        @pl.when(gi == 0)
        def _():
            await_rows(down_full, C * CH - pair_rows(1), cross_down.at[origin_a, 0])

        @pl.when(gi > 0)
        def _():
            await_rows(down_full, C * CH, cross_down.at[origin_a, gi])

    for c in range(C):
        cast(0, c)

        @pl.when(home)
        def _():
            left(0, f, c)

    for c in range(C):
        load(1, c).start()
    token_load.start()

    @pl.when(k < K - 1)
    def _():
        pl.semaphore_wait(ready.at[2], K - 1 - k)
    for c in range(C):
        for b in range(G):
            hand(0, b, c)

    @pl.when(y == 0)
    def _():
        pl.semaphore_wait(ready.at[1], 1)

    @pl.when(a < A - 1)
    def _():
        pl.semaphore_wait(ready.at[0], 1)

    @pl.when(home)
    def _():
        pf, shared = share[0]
        for c in range(C):
            own_chunk(0, c, () if c < pf else (shared if c == pf else 0, W), True, False)

    own(0)
    token_load.wait()
    lax.fori_loop(0, tok // 16, normalize, 0)
    for c in range(C):
        cast(1, c)
        for b in range(G):
            hand(1, b, c)
    tokens()
    mated(0)
    loop(0, A - 2, lambda s: line(0, s))
    own(1)
    line(0, A - 2)
    mated(1)
    line(1, 0)

    await_rows(up_full, A * (NQ * CH - pair_rows(0)), cross.at[0])
    await_rows(nrm, (K - 1) * tok, tok_recv.at[0])

    tile = min(TILE, W)

    def lift(j):
        columns = pl.ds(pl.multiple_of(j * tile, tile), tile)
        lifted = jnp.maximum(jnp.dot(nrm[...], up_full[:, columns], preferred_element_type=jnp.float32), 0.0)
        hid[:, columns] = (lifted * lifted).astype(jnp.bfloat16)
    loop(0, W // tile, lift)

    halves = 2 if R % 128 == 0 else 1

    def part_copy(d, block, columns):
        target = (k + d) % K
        return pltpu.make_async_remote_copy(
            src_ref=stage.at[block, pl.ds(pl.multiple_of(target * tok, 16), tok), columns],
            dst_ref=part.at[d - 1, block, :, columns],
            send_sem=part_send.at[0], recv_sem=part_recv.at[0],
            device_id=at_k(target), device_id_type=MESH)

    def multiply(block, rows, columns):
        value = lax.dot_general(hid[...], down_full[rows, :], (((1,), (1,)), ((), ())),
                                preferred_element_type=jnp.float32)
        stage[block, :, columns] = value.astype(jnp.bfloat16)
        part[K - 1, block, :, columns] = stage[block, mine, columns]
        for d in range(1, K):
            part_copy(d, block, columns).start()

    def lower(origin_a, gi):
        settle_down(origin_a, gi)
        g = (gr + gi) % G
        rows = pl.ds(pl.multiple_of(g * (F * R) + origin_a * (2 * R), 2 * R), 2 * R)
        multiply(origin_a * G + g, rows, pl.ds(0, 2 * R))

    def lower_half(origin_a, side):
        rows = pl.ds(pl.multiple_of(gr * (F * R) + (origin_a * 2 + side) * R, R), R)
        multiply(origin_a * G + gr, rows, pl.ds(pl.multiple_of(side * R, R), R))

    def ends(step):
        @pl.when(a - 1 - (A - 2) >= 0)
        def _():
            step(a - 1 - (A - 2))

        @pl.when(a + 1 + (A - 2) < A)
        def _():
            step(a + 1 + (A - 2))

    def early():
        if halves == 2:
            ends(lambda origin_a: lower_half(origin_a, y))

    def late():
        if halves == 2:
            def step(origin_a):
                settle_down(origin_a, 0)
                lower_half(origin_a, 1 - y)
            ends(step)
        else:
            lower_ring(A - 2, G - 1, G)

    def lower_ring(s, low=0, high=G):
        @pl.when(a - 1 - s >= 0)
        def _():
            loop(low, high, lambda i: lower(a - 1 - s, G - 1 - i))

        @pl.when(a + 1 + s < A)
        def _():
            loop(low, high, lambda i: lower(a + 1 + s, G - 1 - i))

    loop(0, G, lambda i: lower(a, G - 1 - i))
    loop(1, A - 2, lambda s: line(1, s, between=lambda: lower_ring(s - 1)))
    line(1, A - 2, between=lambda: lower_ring(A - 3), eager=lambda: lower_ring(A - 2, 0, G - 1), closing=early)
    late()

    await_rows(part, K - 1, part_recv.at[0])
    await_rows(part, K - 1, part_send.at[0])
    await_rows(nrm, (K - 1) * tok, tok_send.at[0])
    pairs = pair_rows(0) + pair_rows(1)
    await_rows(up_full, 2 * NQ * CH, sendy.at[0])
    for _ in range(A - 1):
        await_rows(up_full, 2 * NQ * CH - pairs, sendy.at[0])

    def drain(sem, rows):
        def step(i, carry):
            await_rows(up_full, rows, sem.at[0])
            return carry
        return step
    lax.fori_loop(0, jnp.where(a > 0, A - a, 0), drain(sendl, 2 * NQ * CH + pairs), 0)
    lax.fori_loop(0, jnp.where(a < A - 1, a + 1, 0), drain(sendr, 2 * NQ * CH + pairs), 0)
    lax.fori_loop(0, jnp.where(home, G - 1, G), drain(send0, 2 * R), 0)


def finish(G, F, up_held, down_held, parts, up_out, down_out, out_ref, summed, sems, out_sem):
    def out(m, i):
        source, target = ((up_held, up_out), (down_held, down_out))[m]
        size = source.shape[0] // SPLIT
        rows = pl.ds(i * size, size)
        return pltpu.make_async_copy(source.at[rows], target.at[rows], sems.at[m, i])

    for m in range(2):
        for i in range(SPLIT):
            out(m, i).start()
    K, blocks, _, wide = parts.shape
    D = out_ref.shape[1]
    for block in range(blocks):
        total = parts[0, block].astype(jnp.float32)
        for i in range(1, K):
            total += parts[i, block].astype(jnp.float32)
        begin = (block % G) * (D // G) + (block // G) * wide
        summed[:, begin:begin + wide] = total.astype(jnp.bfloat16)
    tokens_out = pltpu.make_async_copy(summed, out_ref, out_sem.at[0])
    tokens_out.start()
    for m in range(2):
        for i in range(SPLIT):
            out(m, i).wait()
    tokens_out.wait()


def body(G, F, T, prompt_tokens, up_master, down_master, norm_gain):
    R, width = up_master.shape
    tok = prompt_tokens.shape[0]
    D, W = R * G * F, width // G
    A, K = F // 2, G * T
    C = R // min(CHUNK, R)
    NQ = G * C
    pairs = max(1, max(pf + (shared > 0) for pf, shared in pair_share(NQ, W)))
    bf16 = jnp.bfloat16
    any_space = pl.BlockSpec(memory_space=pl.ANY)
    vmem_space = pl.BlockSpec(memory_space=pltpu.VMEM)
    dma = pltpu.SemaphoreType.DMA
    up_held, down_held, parts = pl.pallas_call(
        functools.partial(kernel, G, F, T),
        name="handoff",
        out_shape=(
            pltpu.MemorySpace.VMEM((D, W), bf16),
            pltpu.MemorySpace.VMEM((D, W), bf16),
            pltpu.MemorySpace.VMEM((K, A * G, tok, 2 * R), bf16),
        ),
        in_specs=[any_space, vmem_space, any_space, any_space],
        out_specs=(vmem_space,) * 3,
        scratch_shapes=[
            pltpu.VMEM((2, R, width), jnp.float32),
            pltpu.VMEM((2, R, width), bf16),
            pltpu.VMEM((tok, D), bf16),
            pltpu.VMEM((K * tok, D), bf16),
            pltpu.VMEM((K * tok, W), bf16),
            pltpu.VMEM((A * G, K * tok, 2 * R), bf16),
            dma((2, A, NQ)), dma((2, A, pairs)), dma((1,)), dma((A, G)),
            dma((1,)), dma((1,)), dma((1,)), dma((1,)), dma((1,)), dma((1,)),
            dma((1,)), dma((1,)), dma((1,)), dma((2, C)), pltpu.SemaphoreType.REGULAR((3,)),
        ],
        compiler_params=pltpu.CompilerParams(
            collective_id=0, has_side_effects=True, vmem_limit_bytes=41 * 1024 * 1024),
    )(prompt_tokens, norm_gain.reshape(1, R), up_master, down_master)
    return pl.pallas_call(
        functools.partial(finish, G, F),
        name="finish",
        out_shape=(
            jax.ShapeDtypeStruct((D, W), bf16),
            jax.ShapeDtypeStruct((D, W), bf16),
            jax.ShapeDtypeStruct((tok, D), bf16),
        ),
        in_specs=[vmem_space] * 3,
        out_specs=(any_space, any_space, any_space),
        scratch_shapes=[pltpu.VMEM((tok, D), bf16), dma((2, SPLIT)), dma((1,))],
        compiler_params=pltpu.CompilerParams(vmem_limit_bytes=16 * 1024 * 1024),
    )(up_held, down_held, parts)


def solution(mesh):
    placed = (
        P(("gr", "fs", "tp"), None),
        P(("gr", "fs"), "tp"),
        P(("gr", "fs"), "tp"),
        P(("gr", "fs")),
    )
    return jax.shard_map(
        functools.partial(body, mesh.shape["gr"], mesh.shape["fs"], mesh.shape["tp"]),
        mesh=mesh,
        in_specs=placed,
        out_specs=(P(None, ("gr", "tp")), P(None, ("gr", "tp")), P(("gr", "fs", "tp"), None)),
        check_vma=False,
    )
```

```python
import functools

import jax
import jax.numpy as jnp
from jax import lax
from jax.experimental import pallas as pl
from jax.experimental.pallas import tpu as pltpu
from jax.sharding import PartitionSpec as P

MESH = pl.DeviceIdType.MESH
CHUNK = 32
TILE = 256
SPLIT = 4


def pair_share(count, width):
    share = []
    for quarters in (count * 5 // 8, count * 6 // 8):
        share.append((quarters // 4, quarters % 4 * (width // 4)))
    return share


def kernel(G, F, T, tok_in, gain_in, up_in, down_in, up_full, down_full, part,
           wide, narrow, raw, nrm, hid, stage,
           recv, dup, cross, cross_down, sendl, sendr, sendy, send0, tok_recv, tok_send,
           part_recv, part_send, local_sem, load_sem, ready):
    gr, f, tp = lax.axis_index("gr"), lax.axis_index("fs"), lax.axis_index("tp")
    full = (up_full, down_full)
    A = F // 2
    a, y = f // 2, f % 2
    mate = a * 2 + 1 - y
    R = up_in.shape[0]
    D, W = up_full.shape
    tok = tok_in.shape[0]
    CH = min(CHUNK, R)
    C = R // CH
    NQ = G * C
    share = pair_share(NQ, W)
    K = G * T
    k = gr * T + tp
    weights = (up_in, down_in)

    def at_k(kk):
        return (kk // T, f, kk % T)

    def load(m, c):
        rows = pl.ds(c * CH, CH) if m == 0 else pl.ds(0, R)
        return pltpu.make_async_copy(weights[m].at[rows], wide.at[m, rows], load_sem.at[c if m == 0 else C])

    load(0, 0).start()
    barrier = pltpu.get_barrier_semaphore()

    @pl.when(a < A - 1)
    def _():
        pl.semaphore_signal(barrier, inc=1, device_id=(gr, f + 2, tp), device_id_type=MESH)

    @pl.when(y == 0)
    def _():
        pl.semaphore_signal(barrier, inc=1, device_id=(gr, mate, tp), device_id_type=MESH)

    for kk in range(1, K):
        @pl.when(kk > k)
        def _():
            pl.semaphore_signal(barrier, inc=1, device_id=at_k(kk), device_id_type=MESH)

    token_load = pltpu.make_async_copy(tok_in, raw, local_sem.at[0])
    for c in range(1, C):
        load(0, c).start()
    partners = (a > 0).astype(jnp.int32) + y + k

    @pl.when(partners > 0)
    def _():
        pl.semaphore_wait(barrier, partners)

    @pl.when(a > 0)
    def _():
        pl.semaphore_signal(ready.at[0], inc=1, device_id=(gr, f - 2, tp), device_id_type=MESH)

    @pl.when(y == 1)
    def _():
        pl.semaphore_signal(ready.at[1], inc=1, device_id=(gr, mate, tp), device_id_type=MESH)

    for kk in range(K - 1):
        @pl.when(kk < k)
        def _():
            pl.semaphore_signal(ready.at[1 + k], inc=1, device_id=at_k(kk), device_id_type=MESH)

    def rows_of(origin, g, c):
        return pl.ds(pl.multiple_of(g * (F * R) + origin * R + c * CH, CH), CH)

    home = k // G == tp

    def cast(m, c):
        rows = pl.ds(c * CH, CH)
        if m == 0 or c == 0:
            load(m, c).wait()
        value = wide[m, rows, :]
        if m == 0:
            value = value * column[c * CH:(c + 1) * CH]
        value = value.astype(jnp.bfloat16)
        narrow[m, rows, :] = value
        for b in range(G):
            @pl.when(tp * G + b == k)
            def _():
                full[m][rows_of(f, gr, c), :] = value[:, b * W:(b + 1) * W]

    def hand(m, b, c):
        kk = tp * G + b
        q = ((gr - kk // T + G) % G) * C + c

        @pl.when(kk != k)
        def _():
            copy = pltpu.make_async_remote_copy(
                src_ref=narrow.at[m, pl.ds(c * CH, CH), pl.ds(b * W, W)],
                dst_ref=full[m].at[rows_of(f, gr, c)],
                send_sem=send0.at[0], recv_sem=recv.at[m, a, q],
                device_id=at_k(kk), device_id_type=MESH)
            copy.start()

    mine = pl.ds(pl.multiple_of(k * tok, 16), tok)

    def tokens():
        for d in range(1, K):
            pltpu.make_async_remote_copy(
                src_ref=nrm.at[mine], dst_ref=nrm.at[mine],
                send_sem=tok_send.at[0], recv_sem=tok_recv.at[0],
                device_id=at_k((k + d) % K), device_id_type=MESH).start()

    def normalize(i, carry):
        values = raw[pl.ds(pl.multiple_of(i * 16, 16), 16), :].astype(jnp.float32)
        center = jnp.mean(values, axis=-1, keepdims=True)
        moved = values - center
        spread = jnp.mean(jnp.square(moved), axis=-1, keepdims=True)
        nrm[pl.ds(pl.multiple_of(k * tok + i * 16, 16), 16), :] = (
            moved * lax.rsqrt(spread + 1e-05)).astype(jnp.bfloat16)
        return carry

    rowed = lax.broadcasted_iota(jnp.int32, (R, R), 0) == lax.broadcasted_iota(jnp.int32, (R, R), 1)
    column = jnp.sum(jnp.where(rowed, gain_in[...], 0.0), axis=1, keepdims=True)

    def chunk(m, origin, q, columns):
        rows = rows_of(origin, (gr + q // C) % G, q % C)
        return full[m].at[rows, pl.ds(columns[0], columns[1] - columns[0])]

    def landing(m, origin_a, side, q):
        if side == "line":
            return recv.at[m, origin_a, q]
        if side == "pair":
            return dup.at[m, origin_a]
        return cross.at[0] if m == 0 else cross_down.at[origin_a, q // C]

    whole = (0, W)

    def send(m, origin, q, sem, side, target, columns=whole):
        ref = chunk(m, origin, q, columns)
        pltpu.make_async_remote_copy(
            src_ref=ref, dst_ref=ref, send_sem=sem.at[0], recv_sem=landing(m, origin // 2, side, q),
            device_id=(gr, target, tp), device_id_type=MESH).start()

    def await_rows(ref, count, sem):
        if count > 0:
            rows = ref.at[pl.ds(0, count)]
            pltpu.make_async_copy(rows, rows, sem).wait()

    def arrived(m, origin, q, side="line", columns=whole):
        ref = chunk(m, origin, q, columns)
        pltpu.make_async_copy(ref, ref, landing(m, origin // 2, side, q)).wait()

    def left(m, origin, q, side="line", columns=whole):
        @pl.when(a > 0)
        def _():
            send(m, origin, q, sendl, side, f - 2, columns)

    def right(m, origin, q, side="line", columns=whole):
        @pl.when(a < A - 1)
        def _():
            send(m, origin, q, sendr, side, f + 2, columns)

    def loop(low, high, step):
        def go(i, carry):
            step(i)
            return carry
        if high > low:
            lax.fori_loop(low, high, go, 0)

    def over_line(m):
        pf, shared = share[m]
        first = pf + (shared > 0)
        return ([(0, pf, ())] if pf else []) + ([(pf, first, (shared, W))] if shared else []), (first, C, whole)

    def over_pair(m):
        pf, shared = share[m]
        return ([(0, pf, whole)] if pf else []) + ([(pf, pf + 1, (0, shared))] if shared else [])

    def across(m, origin, q, columns):
        if columns:
            send(m, origin, q, sendy, "cross", mate, columns)

    def own_across(m, q, columns, pair=True):
        if pair and columns[:1] != (0,):
            send(m, f, q, sendy, "pair", mate, (0, columns[0]) if columns else whole)
        across(m, f, q, columns)

    def own_chunk(m, q, columns, pair=True):
        left(m, f, q)
        right(m, f, q)
        own_across(m, q, columns, pair)

    def own(m):
        def near(columns):
            def step(q):
                @pl.when(jnp.logical_not(home))
                def _():
                    arrived(m, f, q)
                    if m == 0:
                        own_chunk(m, q, columns)
                if m > 0:
                    own_chunk(m, q, columns, False)
            return step

        def far(q):
            arrived(m, f, q)
            own_chunk(m, q, whole)

        shared, rest = over_line(m)
        if m == 0:
            for low, high, columns in shared:
                loop(low, high, near(columns))
            loop(rest[0], rest[1], near(whole))
            loop(C, NQ, far)
        else:
            for low, high, columns in over_pair(m):
                def step(q):
                    @pl.when(jnp.logical_not(home))
                    def _():
                        arrived(m, f, q)
                    send(m, f, q, sendy, "pair", mate, columns)
                loop(low, high, step)

            loop(C, NQ, far)

            def step(columns):
                def go(q):
                    own_chunk(m, q, columns, False)
                return go
            for low, high, columns in shared:
                if columns:
                    loop(low, high, step(columns))
            loop(rest[0], rest[1], near(whole))
            for low, high, columns in shared:
                if not columns:
                    loop(low, high, step(columns))

    def mated(m):
        await_rows(full[m], pair_rows(m), dup.at[m, a])
        for low, high, columns in over_pair(m):
            def step(q):
                left(m, mate, q, "pair", columns)
                right(m, mate, q, "pair", columns)
            loop(low, high, step)

    def line(m, s, between=None, eager=None, closing=None):
        below, above = a - 1 - s, a + 1 + s

        def both(side, columns):
            sent = columns if side == "pair" else whole

            def pass_on(origin, q, onward):
                if side == "line":
                    arrived(m, origin, q)
                onward(m, origin, q, side, sent)
                if side == "line":
                    across(m, origin, q, columns)

            def step(q):
                mine_y = y if side == "line" else 1 - y

                @pl.when(below >= 0)
                def _():
                    pass_on(below * 2 + mine_y, q, right)

                @pl.when(above < A)
                def _():
                    pass_on(above * 2 + mine_y, q, left)
            return step

        shared, rest = over_line(m)
        if m == 0:
            for low, high, columns in shared:
                loop(low, high, both("line", columns))
            loop(rest[0], rest[1], both("line", whole))
            loop(C, NQ, both("line", whole))
        else:
            loop(C, NQ, both("line", whole))
            if between is not None:
                between()
            for low, high, columns in shared:
                if columns:
                    loop(low, high, both("line", columns))
            loop(rest[0], rest[1], both("line", whole))
            if eager is not None:
                eager()
            for low, high, columns in shared:
                if not columns:
                    loop(low, high, both("line", columns))
        if closing is not None:
            closing()
        for origin_a in (below, above):
            @pl.when(jnp.logical_and(origin_a >= 0, origin_a < A))
            def _():
                await_rows(full[m], pair_rows(m), dup.at[m, origin_a])
        for low, high, columns in over_pair(m):
            loop(low, high, both("pair", columns))

    def pair_rows(m):
        pf, shared = share[m]
        return pf * CH + CH * shared // W

    def settle_down(origin_a, gi):
        @pl.when(gi == 0)
        def _():
            await_rows(down_full, C * CH - pair_rows(1), cross_down.at[origin_a, 0])

        @pl.when(gi > 0)
        def _():
            await_rows(down_full, C * CH, cross_down.at[origin_a, gi])

    def sharing(c):
        pf, shared = share[0]
        return () if c < pf else (shared if c == pf else 0, W)

    for c in range(C):
        cast(0, c)

        @pl.when(home)
        def _():
            left(0, f, c)

            @pl.when(y == 1)
            def _():
                own_across(0, c, sharing(c))

    load(1, 0).start()
    token_load.start()

    def meet(kk):
        @pl.when(kk > k)
        def _():
            pl.semaphore_wait(ready.at[1 + kk], 1)

    for b in range(G):
        meet(tp * G + b)
    for c in range(C):
        for b in range(G):
            hand(0, b, c)

    @pl.when(y == 0)
    def _():
        pl.semaphore_wait(ready.at[1], 1)

        @pl.when(home)
        def _():
            for c in range(C):
                own_across(0, c, sharing(c))

    @pl.when(a < A - 1)
    def _():
        pl.semaphore_wait(ready.at[0], 1)

        @pl.when(home)
        def _():
            for c in range(C):
                right(0, f, c)

    own(0)
    token_load.wait()
    lax.fori_loop(0, tok // 16, normalize, 0)
    for c in range(C):
        cast(1, c)
        for b in range(G):
            hand(1, b, c)
    for kk in range(1, K):
        @pl.when(kk // G != tp)
        def _():
            meet(kk)
    tokens()
    mated(0)
    loop(0, A - 2, lambda s: line(0, s))
    own(1)
    line(0, A - 2)
    mated(1)
    line(1, 0)

    await_rows(up_full, A * (NQ * CH - pair_rows(0)), cross.at[0])
    await_rows(nrm, (K - 1) * tok, tok_recv.at[0])

    tile = min(TILE, W)

    def lift(j):
        columns = pl.ds(pl.multiple_of(j * tile, tile), tile)
        lifted = jnp.maximum(jnp.dot(nrm[...], up_full[:, columns], preferred_element_type=jnp.float32), 0.0)
        hid[:, columns] = (lifted * lifted).astype(jnp.bfloat16)
    loop(0, W // tile, lift)

    halves = 2 if R % 128 == 0 else 1

    def part_copy(d, block, columns):
        target = (k + d) % K
        return pltpu.make_async_remote_copy(
            src_ref=stage.at[block, pl.ds(pl.multiple_of(target * tok, 16), tok), columns],
            dst_ref=part.at[d - 1, block, :, columns],
            send_sem=part_send.at[0], recv_sem=part_recv.at[0],
            device_id=at_k(target), device_id_type=MESH)

    def multiply(block, rows, columns):
        value = lax.dot_general(hid[...], down_full[rows, :], (((1,), (1,)), ((), ())),
                                preferred_element_type=jnp.float32)
        stage[block, :, columns] = value.astype(jnp.bfloat16)
        part[K - 1, block, :, columns] = stage[block, mine, columns]
        for d in range(1, K):
            part_copy(d, block, columns).start()

    far = jnp.where(2 * a < A, A - 1, 0)

    def lower(origin_a, gi):
        settle_down(origin_a, gi)
        g = (gr + gi) % G
        rows = pl.ds(pl.multiple_of(g * (F * R) + origin_a * (2 * R), 2 * R), 2 * R)
        multiply(origin_a * G + g, rows, pl.ds(0, 2 * R))

    def lower_half(origin_a, side):
        rows = pl.ds(pl.multiple_of(gr * (F * R) + (origin_a * 2 + side) * R, R), R)
        multiply(origin_a * G + gr, rows, pl.ds(pl.multiple_of(side * R, R), R))

    def at_far(step):
        for end in (0, A - 1):
            @pl.when(far == end)
            def _():
                step(end)

    def early():
        if halves == 2:
            at_far(lambda origin_a: lower_half(origin_a, y))

    def late():
        if halves == 2:
            settle_down(far, 0)
            at_far(lambda origin_a: lower_half(origin_a, 1 - y))
        else:
            lower(far, 0)

    def lower_ring(s, last=True):
        def blocks(origin_a):
            loop(0, G - 1, lambda i: lower(origin_a, G - 1 - i))

            if last:
                @pl.when(origin_a != far)
                def _():
                    lower(origin_a, 0)

        @pl.when(a - 1 - s >= 0)
        def _():
            blocks(a - 1 - s)

        @pl.when(a + 1 + s < A)
        def _():
            blocks(a + 1 + s)

    loop(0, G, lambda i: lower(a, G - 1 - i))
    loop(1, A - 2, lambda s: line(1, s, between=lambda: lower_ring(s - 1)))
    line(1, A - 2, between=lambda: lower_ring(A - 3), eager=lambda: lower_ring(A - 2, False), closing=early)
    late()

    await_rows(part, K - 1, part_recv.at[0])
    await_rows(part, K - 1, part_send.at[0])
    await_rows(nrm, (K - 1) * tok, tok_send.at[0])
    pairs = pair_rows(0) + pair_rows(1)
    await_rows(up_full, 2 * NQ * CH, sendy.at[0])
    for _ in range(A - 1):
        await_rows(up_full, 2 * NQ * CH - pairs, sendy.at[0])

    def drain(sem, rows):
        def step(i, carry):
            await_rows(up_full, rows, sem.at[0])
            return carry
        return step
    lax.fori_loop(0, jnp.where(a > 0, A - a, 0), drain(sendl, 2 * NQ * CH + pairs), 0)
    lax.fori_loop(0, jnp.where(a < A - 1, a + 1, 0), drain(sendr, 2 * NQ * CH + pairs), 0)
    lax.fori_loop(0, jnp.where(home, G - 1, G), drain(send0, 2 * R), 0)


def finish(G, F, up_held, down_held, parts, up_out, down_out, out_ref, summed, sems, out_sem):
    def out(m, i):
        source, target = ((up_held, up_out), (down_held, down_out))[m]
        size = source.shape[0] // SPLIT
        rows = pl.ds(i * size, size)
        return pltpu.make_async_copy(source.at[rows], target.at[rows], sems.at[m, i])

    for m in range(2):
        for i in range(SPLIT):
            out(m, i).start()
    K, blocks, _, wide = parts.shape
    D = out_ref.shape[1]
    for block in range(blocks):
        total = parts[0, block].astype(jnp.float32)
        for i in range(1, K):
            total += parts[i, block].astype(jnp.float32)
        begin = (block % G) * (D // G) + (block // G) * wide
        summed[:, begin:begin + wide] = total.astype(jnp.bfloat16)
    tokens_out = pltpu.make_async_copy(summed, out_ref, out_sem.at[0])
    tokens_out.start()
    for m in range(2):
        for i in range(SPLIT):
            out(m, i).wait()
    tokens_out.wait()


def body(G, F, T, prompt_tokens, up_master, down_master, norm_gain):
    R, width = up_master.shape
    tok = prompt_tokens.shape[0]
    D, W = R * G * F, width // G
    A, K = F // 2, G * T
    C = R // min(CHUNK, R)
    NQ = G * C
    bf16 = jnp.bfloat16
    any_space = pl.BlockSpec(memory_space=pl.ANY)
    vmem_space = pl.BlockSpec(memory_space=pltpu.VMEM)
    dma = pltpu.SemaphoreType.DMA
    up_held, down_held, parts = pl.pallas_call(
        functools.partial(kernel, G, F, T),
        name="handoff",
        out_shape=(
            pltpu.MemorySpace.VMEM((D, W), bf16),
            pltpu.MemorySpace.VMEM((D, W), bf16),
            pltpu.MemorySpace.VMEM((K, A * G, tok, 2 * R), bf16),
        ),
        in_specs=[any_space, vmem_space, any_space, any_space],
        out_specs=(vmem_space,) * 3,
        scratch_shapes=[
            pltpu.VMEM((2, R, width), jnp.float32),
            pltpu.VMEM((2, R, width), bf16),
            pltpu.VMEM((tok, D), bf16),
            pltpu.VMEM((K * tok, D), bf16),
            pltpu.VMEM((K * tok, W), bf16),
            pltpu.VMEM((A * G, K * tok, 2 * R), bf16),
            dma((2, A, NQ)), dma((2, A)), dma((1,)), dma((A, G)),
            dma((1,)), dma((1,)), dma((1,)), dma((1,)), dma((1,)), dma((1,)),
            dma((1,)), dma((1,)), dma((1,)), dma((C + 1,)), pltpu.SemaphoreType.REGULAR((K + 1,)),
        ],
        compiler_params=pltpu.CompilerParams(
            collective_id=0, has_side_effects=True, vmem_limit_bytes=41 * 1024 * 1024),
    )(prompt_tokens, norm_gain.reshape(1, R), up_master, down_master)
    return pl.pallas_call(
        functools.partial(finish, G, F),
        name="finish",
        out_shape=(
            jax.ShapeDtypeStruct((D, W), bf16),
            jax.ShapeDtypeStruct((D, W), bf16),
            jax.ShapeDtypeStruct((tok, D), bf16),
        ),
        in_specs=[vmem_space] * 3,
        out_specs=(any_space, any_space, any_space),
        scratch_shapes=[pltpu.VMEM((tok, D), bf16), dma((2, SPLIT)), dma((1,))],
        compiler_params=pltpu.CompilerParams(vmem_limit_bytes=16 * 1024 * 1024),
    )(up_held, down_held, parts)


def solution(mesh):
    placed = (
        P(("gr", "fs", "tp"), None),
        P(("gr", "fs"), "tp"),
        P(("gr", "fs"), "tp"),
        P(("gr", "fs")),
    )
    return jax.shard_map(
        functools.partial(body, mesh.shape["gr"], mesh.shape["fs"], mesh.shape["tp"]),
        mesh=mesh,
        in_specs=placed,
        out_specs=(P(None, ("gr", "tp")), P(None, ("gr", "tp")), P(("gr", "fs", "tp"), None)),
        check_vma=False,
    )
```

```python
import functools

import jax
import jax.numpy as jnp
from jax import lax
from jax.experimental import pallas as pl
from jax.experimental.pallas import tpu as pltpu
from jax.sharding import PartitionSpec as P

MESH = pl.DeviceIdType.MESH
CHUNK = 32
TILE = 256
SPLIT = 4


def pair_share(count, width):
    share = []
    for eighths in (count * 10 // 8, count * 11 // 8):
        share.append((eighths // 8, eighths % 8 * (width // 8)))
    return share


def kernel(G, F, T, tok_in, gain_in, up_in, down_in, up_full, down_full, part,
           wide, narrow, raw, nrm, hid, stage,
           recv, dup, cross, cross_down, sendl, sendr, sendy, send0, tok_recv, tok_send,
           part_recv, part_send, local_sem, load_sem, ready):
    gr, f, tp = lax.axis_index("gr"), lax.axis_index("fs"), lax.axis_index("tp")
    full = (up_full, down_full)
    A = F // 2
    a, y = f // 2, f % 2
    mate = a * 2 + 1 - y
    R = up_in.shape[0]
    D, W = up_full.shape
    tok = tok_in.shape[0]
    CH = min(CHUNK, R)
    C = R // CH
    NQ = G * C
    share = pair_share(NQ, W)
    K = G * T
    k = gr * T + tp
    weights = (up_in, down_in)

    def at_k(kk):
        return (kk // T, f, kk % T)

    def load(m, c):
        rows = pl.ds(c * CH, CH) if m == 0 else pl.ds(0, R)
        return pltpu.make_async_copy(weights[m].at[rows], wide.at[m, rows], load_sem.at[c if m == 0 else C])

    load(0, 0).start()
    barrier = pltpu.get_barrier_semaphore()

    @pl.when(a < A - 1)
    def _():
        pl.semaphore_signal(barrier, inc=1, device_id=(gr, f + 2, tp), device_id_type=MESH)

    @pl.when(y == 0)
    def _():
        pl.semaphore_signal(barrier, inc=1, device_id=(gr, mate, tp), device_id_type=MESH)

    for kk in range(1, K):
        @pl.when(kk > k)
        def _():
            pl.semaphore_signal(barrier, inc=1, device_id=at_k(kk), device_id_type=MESH)

    token_load = pltpu.make_async_copy(tok_in, raw, local_sem.at[0])
    for c in range(1, C):
        load(0, c).start()
    partners = (a > 0).astype(jnp.int32) + y + k

    @pl.when(partners > 0)
    def _():
        pl.semaphore_wait(barrier, partners)

    @pl.when(a > 0)
    def _():
        pl.semaphore_signal(ready.at[0], inc=1, device_id=(gr, f - 2, tp), device_id_type=MESH)

    @pl.when(y == 1)
    def _():
        pl.semaphore_signal(ready.at[1], inc=1, device_id=(gr, mate, tp), device_id_type=MESH)

    for kk in range(K - 1):
        @pl.when(kk < k)
        def _():
            pl.semaphore_signal(ready.at[1 + k], inc=1, device_id=at_k(kk), device_id_type=MESH)

    def rows_of(origin, g, c):
        return pl.ds(pl.multiple_of(g * (F * R) + origin * R + c * CH, CH), CH)

    home = k // G == tp

    def cast(m, c):
        rows = pl.ds(c * CH, CH)
        if m == 0 or c == 0:
            load(m, c).wait()
        value = wide[m, rows, :]
        if m == 0:
            value = value * column[c * CH:(c + 1) * CH]
        value = value.astype(jnp.bfloat16)
        narrow[m, rows, :] = value
        for b in range(G):
            @pl.when(tp * G + b == k)
            def _():
                full[m][rows_of(f, gr, c), :] = value[:, b * W:(b + 1) * W]

    def hand(m, b, c):
        kk = tp * G + b
        q = ((gr - kk // T + G) % G) * C + c

        @pl.when(kk != k)
        def _():
            copy = pltpu.make_async_remote_copy(
                src_ref=narrow.at[m, pl.ds(c * CH, CH), pl.ds(b * W, W)],
                dst_ref=full[m].at[rows_of(f, gr, c)],
                send_sem=send0.at[0], recv_sem=recv.at[m, a, q],
                device_id=at_k(kk), device_id_type=MESH)
            copy.start()

    mine = pl.ds(pl.multiple_of(k * tok, 16), tok)

    def tokens():
        for d in range(1, K):
            pltpu.make_async_remote_copy(
                src_ref=nrm.at[mine], dst_ref=nrm.at[mine],
                send_sem=tok_send.at[0], recv_sem=tok_recv.at[0],
                device_id=at_k((k + d) % K), device_id_type=MESH).start()

    def normalize(i, carry):
        values = raw[pl.ds(pl.multiple_of(i * 16, 16), 16), :].astype(jnp.float32)
        center = jnp.mean(values, axis=-1, keepdims=True)
        moved = values - center
        spread = jnp.mean(jnp.square(moved), axis=-1, keepdims=True)
        nrm[pl.ds(pl.multiple_of(k * tok + i * 16, 16), 16), :] = (
            moved * lax.rsqrt(spread + 1e-05)).astype(jnp.bfloat16)
        return carry

    rowed = lax.broadcasted_iota(jnp.int32, (R, R), 0) == lax.broadcasted_iota(jnp.int32, (R, R), 1)
    column = jnp.sum(jnp.where(rowed, gain_in[...], 0.0), axis=1, keepdims=True)

    def chunk(m, origin, q, columns):
        rows = rows_of(origin, (gr + q // C) % G, q % C)
        return full[m].at[rows, pl.ds(columns[0], columns[1] - columns[0])]

    def landing(m, origin_a, side, q):
        if side == "line":
            return recv.at[m, origin_a, q]
        if side == "pair":
            return dup.at[m, origin_a]
        return cross.at[0] if m == 0 else cross_down.at[origin_a, q // C]

    whole = (0, W)

    def send(m, origin, q, sem, side, target, columns=whole):
        ref = chunk(m, origin, q, columns)
        pltpu.make_async_remote_copy(
            src_ref=ref, dst_ref=ref, send_sem=sem.at[0], recv_sem=landing(m, origin // 2, side, q),
            device_id=(gr, target, tp), device_id_type=MESH).start()

    def await_rows(ref, count, sem):
        if count > 0:
            rows = ref.at[pl.ds(0, count)]
            if len(ref.shape) == 2 and count % 8:
                rows = ref.at[pl.ds(0, 2 * count), pl.ds(0, ref.shape[1] // 2)]
            pltpu.make_async_copy(rows, rows, sem).wait()

    def arrived(m, origin, q, side="line", columns=whole):
        ref = chunk(m, origin, q, columns)
        pltpu.make_async_copy(ref, ref, landing(m, origin // 2, side, q)).wait()

    def left(m, origin, q, side="line", columns=whole):
        @pl.when(a > 0)
        def _():
            send(m, origin, q, sendl, side, f - 2, columns)

    def right(m, origin, q, side="line", columns=whole):
        @pl.when(a < A - 1)
        def _():
            send(m, origin, q, sendr, side, f + 2, columns)

    def loop(low, high, step):
        def go(i, carry):
            step(i)
            return carry
        if high > low:
            lax.fori_loop(low, high, go, 0)

    def over_line(m):
        pf, shared = share[m]
        first = pf + (shared > 0)
        return ([(0, pf, ())] if pf else []) + ([(pf, first, (shared, W))] if shared else []), (first, C, whole)

    def over_pair(m):
        pf, shared = share[m]
        return ([(0, pf, whole)] if pf else []) + ([(pf, pf + 1, (0, shared))] if shared else [])

    def across(m, origin, q, columns):
        if columns:
            send(m, origin, q, sendy, "cross", mate, columns)

    def own_across(m, q, columns, pair=True):
        if pair and columns[:1] != (0,):
            send(m, f, q, sendy, "pair", mate, (0, columns[0]) if columns else whole)
        across(m, f, q, columns)

    def own_chunk(m, q, columns, pair=True):
        left(m, f, q)
        right(m, f, q)
        own_across(m, q, columns, pair)

    def own(m):
        def near(columns):
            def step(q):
                @pl.when(jnp.logical_not(home))
                def _():
                    arrived(m, f, q)
                    if m == 0:
                        own_chunk(m, q, columns)
                if m > 0:
                    own_chunk(m, q, columns, False)
            return step

        def far(q):
            arrived(m, f, q)
            own_chunk(m, q, whole)

        shared, rest = over_line(m)
        if m == 0:
            for low, high, columns in shared:
                loop(low, high, near(columns))
            loop(rest[0], rest[1], near(whole))
            loop(C, NQ, far)
        else:
            for low, high, columns in over_pair(m):
                def step(q):
                    @pl.when(jnp.logical_not(home))
                    def _():
                        arrived(m, f, q)
                    send(m, f, q, sendy, "pair", mate, columns)
                loop(low, high, step)

            loop(C, NQ, far)

            def step(columns):
                def go(q):
                    own_chunk(m, q, columns, False)
                return go
            for low, high, columns in shared:
                if columns:
                    loop(low, high, step(columns))
            loop(rest[0], rest[1], near(whole))
            for low, high, columns in shared:
                if not columns:
                    loop(low, high, step(columns))

    def mated(m):
        await_rows(full[m], pair_rows(m), dup.at[m, a])
        for low, high, columns in over_pair(m):
            def step(q):
                left(m, mate, q, "pair", columns)
                right(m, mate, q, "pair", columns)
            loop(low, high, step)

    def line(m, s, between=None, eager=None, closing=None):
        below, above = a - 1 - s, a + 1 + s

        def both(side, columns):
            sent = columns if side == "pair" else whole

            def pass_on(origin, q, onward):
                if side == "line":
                    arrived(m, origin, q)
                onward(m, origin, q, side, sent)
                if side == "line":
                    across(m, origin, q, columns)

            def step(q):
                mine_y = y if side == "line" else 1 - y

                @pl.when(below >= 0)
                def _():
                    pass_on(below * 2 + mine_y, q, right)

                @pl.when(above < A)
                def _():
                    pass_on(above * 2 + mine_y, q, left)
            return step

        shared, rest = over_line(m)
        if m == 0:
            for low, high, columns in shared:
                loop(low, high, both("line", columns))
            loop(rest[0], rest[1], both("line", whole))
            loop(C, NQ, both("line", whole))
        else:
            loop(C, NQ, both("line", whole))
            if between is not None:
                between()
            for low, high, columns in shared:
                if columns:
                    loop(low, high, both("line", columns))
            loop(rest[0], rest[1], both("line", whole))
            if eager is not None:
                eager()
            for low, high, columns in shared:
                if not columns:
                    loop(low, high, both("line", columns))
        if closing is not None:
            closing()
        for origin_a in (below, above):
            @pl.when(jnp.logical_and(origin_a >= 0, origin_a < A))
            def _():
                await_rows(full[m], pair_rows(m), dup.at[m, origin_a])
        for low, high, columns in over_pair(m):
            loop(low, high, both("pair", columns))

    def pair_rows(m):
        pf, shared = share[m]
        return pf * CH + CH * shared // W

    def settle_down(origin_a, gi):
        @pl.when(gi == 0)
        def _():
            await_rows(down_full, C * CH - pair_rows(1), cross_down.at[origin_a, 0])

        @pl.when(gi > 0)
        def _():
            await_rows(down_full, C * CH, cross_down.at[origin_a, gi])

    def sharing(c):
        pf, shared = share[0]
        return () if c < pf else (shared if c == pf else 0, W)

    for c in range(C):
        cast(0, c)

        @pl.when(home)
        def _():
            left(0, f, c)

            @pl.when(y == 1)
            def _():
                own_across(0, c, sharing(c))

    load(1, 0).start()
    token_load.start()

    def meet(kk):
        @pl.when(kk > k)
        def _():
            pl.semaphore_wait(ready.at[1 + kk], 1)

    for b in range(G):
        meet(tp * G + b)
    for c in range(C):
        for b in range(G):
            hand(0, b, c)

    @pl.when(y == 0)
    def _():
        pl.semaphore_wait(ready.at[1], 1)

        @pl.when(home)
        def _():
            for c in range(C):
                own_across(0, c, sharing(c))

    @pl.when(a < A - 1)
    def _():
        pl.semaphore_wait(ready.at[0], 1)

        @pl.when(home)
        def _():
            for c in range(C):
                right(0, f, c)

    own(0)
    token_load.wait()
    lax.fori_loop(0, tok // 16, normalize, 0)
    for c in range(C):
        cast(1, c)
        for b in range(G):
            hand(1, b, c)
    for kk in range(1, K):
        @pl.when(kk // G != tp)
        def _():
            meet(kk)
    tokens()
    mated(0)
    loop(0, A - 2, lambda s: line(0, s))
    own(1)
    line(0, A - 2)
    mated(1)
    line(1, 0)

    await_rows(up_full, A * (NQ * CH - pair_rows(0)), cross.at[0])
    await_rows(nrm, (K - 1) * tok, tok_recv.at[0])

    tile = min(TILE, W)

    def lift(j):
        columns = pl.ds(pl.multiple_of(j * tile, tile), tile)
        lifted = jnp.maximum(jnp.dot(nrm[...], up_full[:, columns], preferred_element_type=jnp.float32), 0.0)
        hid[:, columns] = (lifted * lifted).astype(jnp.bfloat16)
    loop(0, W // tile, lift)

    halves = 2 if R % 128 == 0 else 1

    def part_copy(d, block, columns):
        target = (k + d) % K
        return pltpu.make_async_remote_copy(
            src_ref=stage.at[block, pl.ds(pl.multiple_of(target * tok, 16), tok), columns],
            dst_ref=part.at[d - 1, block, :, columns],
            send_sem=part_send.at[0], recv_sem=part_recv.at[0],
            device_id=at_k(target), device_id_type=MESH)

    def multiply(block, rows, columns):
        value = lax.dot_general(hid[...], down_full[rows, :], (((1,), (1,)), ((), ())),
                                preferred_element_type=jnp.float32)
        stage[block, :, columns] = value.astype(jnp.bfloat16)
        for d in range(1, K):
            part_copy(d, block, columns).start()
        part[K - 1, block, :, columns] = stage[block, mine, columns]

    far = jnp.where(2 * a < A, A - 1, 0)

    def lower(origin_a, gi):
        settle_down(origin_a, gi)
        g = (gr + gi) % G
        rows = pl.ds(pl.multiple_of(g * (F * R) + origin_a * (2 * R), 2 * R), 2 * R)
        multiply(origin_a * G + g, rows, pl.ds(0, 2 * R))

    def lower_half(origin_a, side):
        rows = pl.ds(pl.multiple_of(gr * (F * R) + (origin_a * 2 + side) * R, R), R)
        multiply(origin_a * G + gr, rows, pl.ds(pl.multiple_of(side * R, R), R))

    def at_far(step):
        for end in (0, A - 1):
            @pl.when(far == end)
            def _():
                step(end)

    def early():
        if halves == 2:
            at_far(lambda origin_a: lower_half(origin_a, y))

    def late():
        if halves == 2:
            settle_down(far, 0)
            at_far(lambda origin_a: lower_half(origin_a, 1 - y))
        else:
            lower(far, 0)

    def lower_ring(s, last=True):
        def blocks(origin_a):
            loop(0, G - 1, lambda i: lower(origin_a, G - 1 - i))

            if last:
                @pl.when(origin_a != far)
                def _():
                    lower(origin_a, 0)

        @pl.when(a - 1 - s >= 0)
        def _():
            blocks(a - 1 - s)

        @pl.when(a + 1 + s < A)
        def _():
            blocks(a + 1 + s)

    loop(0, G, lambda i: lower(a, G - 1 - i))
    loop(1, A - 2, lambda s: line(1, s, between=lambda: lower_ring(s - 1)))
    line(1, A - 2, between=lambda: lower_ring(A - 3), eager=lambda: lower_ring(A - 2, False), closing=early)
    late()

    await_rows(nrm, (K - 1) * tok, tok_send.at[0])
    pairs = pair_rows(0) + pair_rows(1)
    await_rows(up_full, 2 * NQ * CH, sendy.at[0])
    for _ in range(A - 1):
        await_rows(up_full, 2 * NQ * CH - pairs, sendy.at[0])

    def drain(sem, rows):
        def step(i, carry):
            await_rows(up_full, rows, sem.at[0])
            return carry
        return step
    lax.fori_loop(0, jnp.where(a > 0, A - a, 0), drain(sendl, 2 * NQ * CH + pairs), 0)
    lax.fori_loop(0, jnp.where(a < A - 1, a + 1, 0), drain(sendr, 2 * NQ * CH + pairs), 0)
    lax.fori_loop(0, jnp.where(home, G - 1, G), drain(send0, 2 * R), 0)
    await_rows(part, K - 1, part_recv.at[0])
    await_rows(part, K - 1, part_send.at[0])


def finish(G, F, up_held, down_held, parts, up_out, down_out, out_ref, summed, sems, out_sem):
    def out(m, i):
        source, target = ((up_held, up_out), (down_held, down_out))[m]
        size = source.shape[0] // SPLIT
        rows = pl.ds(i * size, size)
        return pltpu.make_async_copy(source.at[rows], target.at[rows], sems.at[m, i])

    for m in range(2):
        for i in range(SPLIT):
            out(m, i).start()
    K, blocks, _, wide = parts.shape
    D = out_ref.shape[1]
    for block in range(blocks):
        total = parts[0, block].astype(jnp.float32)
        for i in range(1, K):
            total += parts[i, block].astype(jnp.float32)
        begin = (block % G) * (D // G) + (block // G) * wide
        summed[:, begin:begin + wide] = total.astype(jnp.bfloat16)
    tokens_out = pltpu.make_async_copy(summed, out_ref, out_sem.at[0])
    tokens_out.start()
    for m in range(2):
        for i in range(SPLIT):
            out(m, i).wait()
    tokens_out.wait()


def body(G, F, T, prompt_tokens, up_master, down_master, norm_gain):
    R, width = up_master.shape
    tok = prompt_tokens.shape[0]
    D, W = R * G * F, width // G
    A, K = F // 2, G * T
    C = R // min(CHUNK, R)
    NQ = G * C
    bf16 = jnp.bfloat16
    any_space = pl.BlockSpec(memory_space=pl.ANY)
    vmem_space = pl.BlockSpec(memory_space=pltpu.VMEM)
    dma = pltpu.SemaphoreType.DMA
    up_held, down_held, parts = pl.pallas_call(
        functools.partial(kernel, G, F, T),
        name="handoff",
        out_shape=(
            pltpu.MemorySpace.VMEM((D, W), bf16),
            pltpu.MemorySpace.VMEM((D, W), bf16),
            pltpu.MemorySpace.VMEM((K, A * G, tok, 2 * R), bf16),
        ),
        in_specs=[any_space, vmem_space, any_space, any_space],
        out_specs=(vmem_space,) * 3,
        scratch_shapes=[
            pltpu.VMEM((2, R, width), jnp.float32),
            pltpu.VMEM((2, R, width), bf16),
            pltpu.VMEM((tok, D), bf16),
            pltpu.VMEM((K * tok, D), bf16),
            pltpu.VMEM((K * tok, W), bf16),
            pltpu.VMEM((A * G, K * tok, 2 * R), bf16),
            dma((2, A, NQ)), dma((2, A)), dma((1,)), dma((A, G)),
            dma((1,)), dma((1,)), dma((1,)), dma((1,)), dma((1,)), dma((1,)),
            dma((1,)), dma((1,)), dma((1,)), dma((C + 1,)), pltpu.SemaphoreType.REGULAR((K + 1,)),
        ],
        compiler_params=pltpu.CompilerParams(
            collective_id=0, has_side_effects=True, vmem_limit_bytes=41 * 1024 * 1024),
    )(prompt_tokens, norm_gain.reshape(1, R), up_master, down_master)
    return pl.pallas_call(
        functools.partial(finish, G, F),
        name="finish",
        out_shape=(
            jax.ShapeDtypeStruct((D, W), bf16),
            jax.ShapeDtypeStruct((D, W), bf16),
            jax.ShapeDtypeStruct((tok, D), bf16),
        ),
        in_specs=[vmem_space] * 3,
        out_specs=(any_space, any_space, any_space),
        scratch_shapes=[pltpu.VMEM((tok, D), bf16), dma((2, SPLIT)), dma((1,))],
        compiler_params=pltpu.CompilerParams(vmem_limit_bytes=16 * 1024 * 1024),
    )(up_held, down_held, parts)


def solution(mesh):
    placed = (
        P(("gr", "fs", "tp"), None),
        P(("gr", "fs"), "tp"),
        P(("gr", "fs"), "tp"),
        P(("gr", "fs")),
    )
    return jax.shard_map(
        functools.partial(body, mesh.shape["gr"], mesh.shape["fs"], mesh.shape["tp"]),
        mesh=mesh,
        in_specs=placed,
        out_specs=(P(None, ("gr", "tp")), P(None, ("gr", "tp")), P(("gr", "fs", "tp"), None)),
        check_vma=False,
    )
```

```python
import functools

import jax
import jax.numpy as jnp
from jax import lax
from jax.experimental import pallas as pl
from jax.experimental.pallas import tpu as pltpu
from jax.sharding import PartitionSpec as P

MESH = pl.DeviceIdType.MESH
CHUNK = 32
TILE = 256
SPLIT = 4


def pair_share(count, width):
    share = []
    for eighths in (count * 10 // 8, count * 11 // 8):
        share.append((eighths // 8, eighths % 8 * (width // 8)))
    return share


def kernel(G, F, T, tok_in, gain_in, up_in, down_in, up_full, down_full, part,
           wide, narrow, raw, nrm, hid, stage,
           recv, dup, cross, cross_down, sendl, sendr, sendy, send0, tok_recv, tok_send,
           part_recv, part_send, local_sem, load_sem, ready):
    gr, f, tp = lax.axis_index("gr"), lax.axis_index("fs"), lax.axis_index("tp")
    full = (up_full, down_full)
    A = F // 2
    a, y = f // 2, f % 2
    mate = a * 2 + 1 - y
    R = up_in.shape[0]
    D, W = up_full.shape
    tok = tok_in.shape[0]
    CH = min(CHUNK, R)
    C = R // CH
    NQ = G * C
    share = pair_share(NQ, W)
    K = G * T
    k = gr * T + tp
    weights = (up_in, down_in)

    def at_k(kk):
        return (kk // T, f, kk % T)

    def load(m, c):
        rows = pl.ds(c * CH, CH) if m == 0 else pl.ds(0, R)
        return pltpu.make_async_copy(weights[m].at[rows], wide.at[m, rows], load_sem.at[c if m == 0 else C])

    load(0, 0).start()
    barrier = pltpu.get_barrier_semaphore()

    @pl.when(a < A - 1)
    def _():
        pl.semaphore_signal(barrier, inc=1, device_id=(gr, f + 2, tp), device_id_type=MESH)

    @pl.when(y == 0)
    def _():
        pl.semaphore_signal(barrier, inc=1, device_id=(gr, mate, tp), device_id_type=MESH)

    for kk in range(1, K):
        @pl.when(kk > k)
        def _():
            pl.semaphore_signal(barrier, inc=1, device_id=at_k(kk), device_id_type=MESH)

    token_load = pltpu.make_async_copy(tok_in, raw, local_sem.at[0])
    for c in range(1, C):
        load(0, c).start()
    partners = (a > 0).astype(jnp.int32) + y + k

    @pl.when(partners > 0)
    def _():
        pl.semaphore_wait(barrier, partners)

    @pl.when(a > 0)
    def _():
        pl.semaphore_signal(ready.at[0], inc=1, device_id=(gr, f - 2, tp), device_id_type=MESH)

    @pl.when(y == 1)
    def _():
        pl.semaphore_signal(ready.at[1], inc=1, device_id=(gr, mate, tp), device_id_type=MESH)

    for kk in range(K - 1):
        @pl.when(kk < k)
        def _():
            pl.semaphore_signal(ready.at[1 + k], inc=1, device_id=at_k(kk), device_id_type=MESH)

    def rows_of(origin, g, c):
        return pl.ds(pl.multiple_of(g * (F * R) + origin * R + c * CH, CH), CH)

    home = k // G == tp

    def cast(m, c):
        rows = pl.ds(c * CH, CH)
        if m == 0 or c == 0:
            load(m, c).wait()
        value = wide[m, rows, :]
        if m == 0:
            value = value * column[c * CH:(c + 1) * CH]
        value = value.astype(jnp.bfloat16)
        narrow[m, rows, :] = value
        for b in range(G):
            @pl.when(tp * G + b == k)
            def _():
                full[m][rows_of(f, gr, c), :] = value[:, b * W:(b + 1) * W]

    batch = 2 if C % 2 == 0 else 1

    def slot(q):
        return jnp.where(q < C, q, C + (q - C) // batch)

    def hand(m, b, c):
        kk = tp * G + b
        q = ((gr - kk // T + G) % G) * C + c

        @pl.when(kk != k)
        def _():
            copy = pltpu.make_async_remote_copy(
                src_ref=narrow.at[m, pl.ds(c * CH, CH), pl.ds(b * W, W)],
                dst_ref=full[m].at[rows_of(f, gr, c)],
                send_sem=send0.at[0], recv_sem=recv.at[m, a, slot(q)],
                device_id=at_k(kk), device_id_type=MESH)
            copy.start()

    mine = pl.ds(pl.multiple_of(k * tok, 16), tok)

    def tokens():
        for d in range(1, K):
            pltpu.make_async_remote_copy(
                src_ref=nrm.at[mine], dst_ref=nrm.at[mine],
                send_sem=tok_send.at[0], recv_sem=tok_recv.at[0],
                device_id=at_k((k + d) % K), device_id_type=MESH).start()

    def normalize(i, carry):
        values = raw[pl.ds(pl.multiple_of(i * 16, 16), 16), :].astype(jnp.float32)
        center = jnp.mean(values, axis=-1, keepdims=True)
        moved = values - center
        spread = jnp.mean(jnp.square(moved), axis=-1, keepdims=True)
        nrm[pl.ds(pl.multiple_of(k * tok + i * 16, 16), 16), :] = (
            moved * lax.rsqrt(spread + 1e-05)).astype(jnp.bfloat16)
        return carry

    rowed = lax.broadcasted_iota(jnp.int32, (R, R), 0) == lax.broadcasted_iota(jnp.int32, (R, R), 1)
    column = jnp.sum(jnp.where(rowed, gain_in[...], 0.0), axis=1, keepdims=True)

    def chunk(m, origin, q, columns):
        rows = rows_of(origin, (gr + q // C) % G, q % C)
        return full[m].at[rows, pl.ds(columns[0], columns[1] - columns[0])]

    def landing(m, origin_a, side, q):
        if side == "line":
            return recv.at[m, origin_a, slot(q)]
        if side == "pair":
            return dup.at[m, origin_a]
        return cross.at[0] if m == 0 else cross_down.at[origin_a, q // C]

    whole = (0, W)

    def send(m, origin, q, sem, side, target, columns=whole):
        ref = chunk(m, origin, q, columns)
        pltpu.make_async_remote_copy(
            src_ref=ref, dst_ref=ref, send_sem=sem.at[0], recv_sem=landing(m, origin // 2, side, q),
            device_id=(gr, target, tp), device_id_type=MESH).start()

    def await_rows(ref, count, sem):
        if count > 0:
            rows = ref.at[pl.ds(0, count)]
            if len(ref.shape) == 2 and count % 8:
                rows = ref.at[pl.ds(0, 2 * count), pl.ds(0, ref.shape[1] // 2)]
            pltpu.make_async_copy(rows, rows, sem).wait()

    def arrived(m, origin, q):
        sem = landing(m, origin // 2, "line", q)

        @pl.when(q < C)
        def _():
            ref = chunk(m, origin, q, whole)
            pltpu.make_async_copy(ref, ref, sem).wait()

        @pl.when(jnp.logical_and(q >= C, (q - C) % batch == 0))
        def _():
            await_rows(full[m], batch * CH, sem)

    def left(m, origin, q, side="line", columns=whole):
        @pl.when(a > 0)
        def _():
            send(m, origin, q, sendl, side, f - 2, columns)

    def right(m, origin, q, side="line", columns=whole):
        @pl.when(a < A - 1)
        def _():
            send(m, origin, q, sendr, side, f + 2, columns)

    def loop(low, high, step):
        def go(i, carry):
            step(i)
            return carry
        if high > low:
            lax.fori_loop(low, high, go, 0)

    def over_line(m):
        pf, shared = share[m]
        first = pf + (shared > 0)
        return ([(0, pf, ())] if pf else []) + ([(pf, first, (shared, W))] if shared else []), (first, C, whole)

    def over_pair(m):
        pf, shared = share[m]
        return ([(0, pf, whole)] if pf else []) + ([(pf, pf + 1, (0, shared))] if shared else [])

    def across(m, origin, q, columns):
        if columns:
            send(m, origin, q, sendy, "cross", mate, columns)

    def own_across(m, q, columns, pair=True):
        if pair and columns[:1] != (0,):
            send(m, f, q, sendy, "pair", mate, (0, columns[0]) if columns else whole)
        across(m, f, q, columns)

    def own_chunk(m, q, columns, pair=True):
        left(m, f, q)
        right(m, f, q)
        own_across(m, q, columns, pair)

    def own(m):
        def near(columns):
            def step(q):
                @pl.when(jnp.logical_not(home))
                def _():
                    arrived(m, f, q)
                    if m == 0:
                        own_chunk(m, q, columns)
                if m > 0:
                    own_chunk(m, q, columns, False)
            return step

        def far(q):
            arrived(m, f, q)
            own_chunk(m, q, whole)

        shared, rest = over_line(m)
        if m == 0:
            for low, high, columns in shared:
                loop(low, high, near(columns))
            loop(rest[0], rest[1], near(whole))
            loop(C, NQ, far)
        else:
            for low, high, columns in over_pair(m):
                def step(q):
                    @pl.when(jnp.logical_not(home))
                    def _():
                        arrived(m, f, q)
                    send(m, f, q, sendy, "pair", mate, columns)
                loop(low, high, step)

            loop(C, NQ, far)

            def step(columns):
                def go(q):
                    own_chunk(m, q, columns, False)
                return go
            for low, high, columns in shared:
                if columns:
                    loop(low, high, step(columns))
            loop(rest[0], rest[1], near(whole))
            for low, high, columns in shared:
                if not columns:
                    loop(low, high, step(columns))

    def mated(m):
        await_rows(full[m], pair_rows(m), dup.at[m, a])
        for low, high, columns in over_pair(m):
            def step(q):
                left(m, mate, q, "pair", columns)
                right(m, mate, q, "pair", columns)
            loop(low, high, step)

    def line(m, s, between=None, eager=None, closing=None):
        below, above = a - 1 - s, a + 1 + s

        def both(side, columns):
            sent = columns if side == "pair" else whole

            def pass_on(origin, q, onward):
                if side == "line":
                    arrived(m, origin, q)
                onward(m, origin, q, side, sent)
                if side == "line":
                    across(m, origin, q, columns)

            def step(q):
                mine_y = y if side == "line" else 1 - y

                @pl.when(below >= 0)
                def _():
                    pass_on(below * 2 + mine_y, q, right)

                @pl.when(above < A)
                def _():
                    pass_on(above * 2 + mine_y, q, left)
            return step

        shared, rest = over_line(m)
        if m == 0:
            for low, high, columns in shared:
                loop(low, high, both("line", columns))
            loop(rest[0], rest[1], both("line", whole))
            loop(C, NQ, both("line", whole))
        else:
            loop(C, NQ, both("line", whole))
            if between is not None:
                between()
            for low, high, columns in shared:
                if columns:
                    loop(low, high, both("line", columns))
            loop(rest[0], rest[1], both("line", whole))
            if eager is not None:
                eager()
            for low, high, columns in shared:
                if not columns:
                    loop(low, high, both("line", columns))
        if closing is not None:
            closing()
        for origin_a in (below, above):
            @pl.when(jnp.logical_and(origin_a >= 0, origin_a < A))
            def _():
                await_rows(full[m], pair_rows(m), dup.at[m, origin_a])
        for low, high, columns in over_pair(m):
            loop(low, high, both("pair", columns))

    def pair_rows(m):
        pf, shared = share[m]
        return pf * CH + CH * shared // W

    def settle_down(origin_a, gi):
        @pl.when(gi == 0)
        def _():
            await_rows(down_full, C * CH - pair_rows(1), cross_down.at[origin_a, 0])

        @pl.when(gi > 0)
        def _():
            await_rows(down_full, C * CH, cross_down.at[origin_a, gi])

    def sharing(c):
        pf, shared = share[0]
        return () if c < pf else (shared if c == pf else 0, W)

    for c in range(C):
        cast(0, c)

        @pl.when(home)
        def _():
            left(0, f, c)

            @pl.when(y == 1)
            def _():
                own_across(0, c, sharing(c))

    load(1, 0).start()
    token_load.start()

    def meet(kk):
        @pl.when(kk > k)
        def _():
            pl.semaphore_wait(ready.at[1 + kk], 1)

    for b in range(G):
        meet(tp * G + b)
    for c in range(C):
        for b in range(G):
            hand(0, b, c)

    @pl.when(y == 0)
    def _():
        pl.semaphore_wait(ready.at[1], 1)

        @pl.when(home)
        def _():
            for c in range(C):
                own_across(0, c, sharing(c))

    @pl.when(a < A - 1)
    def _():
        pl.semaphore_wait(ready.at[0], 1)

        @pl.when(home)
        def _():
            for c in range(C):
                right(0, f, c)

    own(0)
    token_load.wait()
    lax.fori_loop(0, tok // 16, normalize, 0)
    for c in range(C):
        cast(1, c)
        for b in range(G):
            hand(1, b, c)
    for kk in range(1, K):
        @pl.when(kk // G != tp)
        def _():
            meet(kk)
    tokens()
    mated(0)
    loop(0, A - 2, lambda s: line(0, s))
    own(1)
    line(0, A - 2)
    mated(1)
    line(1, 0)

    await_rows(up_full, A * (NQ * CH - pair_rows(0)), cross.at[0])
    await_rows(nrm, (K - 1) * tok, tok_recv.at[0])

    tile = min(TILE, W)

    def lift(j):
        columns = pl.ds(pl.multiple_of(j * tile, tile), tile)
        lifted = jnp.maximum(jnp.dot(nrm[...], up_full[:, columns], preferred_element_type=jnp.float32), 0.0)
        hid[:, columns] = (lifted * lifted).astype(jnp.bfloat16)
    loop(0, W // tile, lift)

    halves = 2 if R % 128 == 0 else 1

    def part_copy(d, block, columns):
        target = (k + d) % K
        return pltpu.make_async_remote_copy(
            src_ref=stage.at[block, pl.ds(pl.multiple_of(target * tok, 16), tok), columns],
            dst_ref=part.at[d - 1, block, :, columns],
            send_sem=part_send.at[0], recv_sem=part_recv.at[0],
            device_id=at_k(target), device_id_type=MESH)

    def multiply(block, rows, columns):
        value = lax.dot_general(hid[...], down_full[rows, :], (((1,), (1,)), ((), ())),
                                preferred_element_type=jnp.float32)
        stage[block, :, columns] = value.astype(jnp.bfloat16)
        for d in range(1, K):
            part_copy(d, block, columns).start()
        part[K - 1, block, :, columns] = stage[block, mine, columns]

    far = jnp.where(2 * a < A, A - 1, 0)

    def lower(origin_a, gi):
        settle_down(origin_a, gi)
        g = (gr + gi) % G
        rows = pl.ds(pl.multiple_of(g * (F * R) + origin_a * (2 * R), 2 * R), 2 * R)
        multiply(origin_a * G + g, rows, pl.ds(0, 2 * R))

    def lower_half(origin_a, side):
        rows = pl.ds(pl.multiple_of(gr * (F * R) + (origin_a * 2 + side) * R, R), R)
        multiply(origin_a * G + gr, rows, pl.ds(pl.multiple_of(side * R, R), R))

    def at_far(step):
        for end in (0, A - 1):
            @pl.when(far == end)
            def _():
                step(end)

    def early():
        if halves == 2:
            at_far(lambda origin_a: lower_half(origin_a, y))

    def late():
        if halves == 2:
            settle_down(far, 0)
            at_far(lambda origin_a: lower_half(origin_a, 1 - y))
        else:
            lower(far, 0)

    def lower_ring(s, last=True):
        def blocks(origin_a):
            loop(0, G - 1, lambda i: lower(origin_a, G - 1 - i))

            if last:
                @pl.when(origin_a != far)
                def _():
                    lower(origin_a, 0)

        @pl.when(a - 1 - s >= 0)
        def _():
            blocks(a - 1 - s)

        @pl.when(a + 1 + s < A)
        def _():
            blocks(a + 1 + s)

    loop(0, G, lambda i: lower(a, G - 1 - i))
    loop(1, A - 2, lambda s: line(1, s, between=lambda: lower_ring(s - 1)))
    line(1, A - 2, between=lambda: lower_ring(A - 3), eager=lambda: lower_ring(A - 2, False), closing=early)
    late()

    await_rows(nrm, (K - 1) * tok, tok_send.at[0])
    pairs = pair_rows(0) + pair_rows(1)
    await_rows(up_full, 2 * NQ * CH, sendy.at[0])
    for _ in range(A - 1):
        await_rows(up_full, 2 * NQ * CH - pairs, sendy.at[0])

    def drain(sem, rows):
        def step(i, carry):
            await_rows(up_full, rows, sem.at[0])
            return carry
        return step
    lax.fori_loop(0, jnp.where(a > 0, A - a, 0), drain(sendl, 2 * NQ * CH + pairs), 0)
    lax.fori_loop(0, jnp.where(a < A - 1, a + 1, 0), drain(sendr, 2 * NQ * CH + pairs), 0)
    lax.fori_loop(0, jnp.where(home, G - 1, G), drain(send0, 2 * R), 0)
    await_rows(part, K - 1, part_recv.at[0])
    await_rows(part, K - 1, part_send.at[0])


def finish(G, F, up_held, down_held, parts, up_out, down_out, out_ref, summed, sems, out_sem):
    def out(m, i):
        source, target = ((up_held, up_out), (down_held, down_out))[m]
        size = source.shape[0] // SPLIT
        rows = pl.ds(i * size, size)
        return pltpu.make_async_copy(source.at[rows], target.at[rows], sems.at[m, i])

    for m in range(2):
        for i in range(SPLIT):
            out(m, i).start()
    K, blocks, _, wide = parts.shape
    D = out_ref.shape[1]
    for block in range(blocks):
        total = parts[0, block].astype(jnp.float32)
        for i in range(1, K):
            total += parts[i, block].astype(jnp.float32)
        begin = (block % G) * (D // G) + (block // G) * wide
        summed[:, begin:begin + wide] = total.astype(jnp.bfloat16)
    tokens_out = pltpu.make_async_copy(summed, out_ref, out_sem.at[0])
    tokens_out.start()
    for m in range(2):
        for i in range(SPLIT):
            out(m, i).wait()
    tokens_out.wait()


def body(G, F, T, prompt_tokens, up_master, down_master, norm_gain):
    R, width = up_master.shape
    tok = prompt_tokens.shape[0]
    D, W = R * G * F, width // G
    A, K = F // 2, G * T
    C = R // min(CHUNK, R)
    NQ = G * C
    bf16 = jnp.bfloat16
    any_space = pl.BlockSpec(memory_space=pl.ANY)
    vmem_space = pl.BlockSpec(memory_space=pltpu.VMEM)
    dma = pltpu.SemaphoreType.DMA
    up_held, down_held, parts = pl.pallas_call(
        functools.partial(kernel, G, F, T),
        name="handoff",
        out_shape=(
            pltpu.MemorySpace.VMEM((D, W), bf16),
            pltpu.MemorySpace.VMEM((D, W), bf16),
            pltpu.MemorySpace.VMEM((K, A * G, tok, 2 * R), bf16),
        ),
        in_specs=[any_space, vmem_space, any_space, any_space],
        out_specs=(vmem_space,) * 3,
        scratch_shapes=[
            pltpu.VMEM((2, R, width), jnp.float32),
            pltpu.VMEM((2, R, width), bf16),
            pltpu.VMEM((tok, D), bf16),
            pltpu.VMEM((K * tok, D), bf16),
            pltpu.VMEM((K * tok, W), bf16),
            pltpu.VMEM((A * G, K * tok, 2 * R), bf16),
            dma((2, A, C + (NQ - C) // (2 if C % 2 == 0 else 1))), dma((2, A)), dma((1,)), dma((A, G)),
            dma((1,)), dma((1,)), dma((1,)), dma((1,)), dma((1,)), dma((1,)),
            dma((1,)), dma((1,)), dma((1,)), dma((C + 1,)), pltpu.SemaphoreType.REGULAR((K + 1,)),
        ],
        compiler_params=pltpu.CompilerParams(
            collective_id=0, has_side_effects=True, vmem_limit_bytes=41 * 1024 * 1024),
    )(prompt_tokens, norm_gain.reshape(1, R), up_master, down_master)
    return pl.pallas_call(
        functools.partial(finish, G, F),
        name="finish",
        out_shape=(
            jax.ShapeDtypeStruct((D, W), bf16),
            jax.ShapeDtypeStruct((D, W), bf16),
            jax.ShapeDtypeStruct((tok, D), bf16),
        ),
        in_specs=[vmem_space] * 3,
        out_specs=(any_space, any_space, any_space),
        scratch_shapes=[pltpu.VMEM((tok, D), bf16), dma((2, SPLIT)), dma((1,))],
        compiler_params=pltpu.CompilerParams(vmem_limit_bytes=16 * 1024 * 1024),
    )(up_held, down_held, parts)


def solution(mesh):
    placed = (
        P(("gr", "fs", "tp"), None),
        P(("gr", "fs"), "tp"),
        P(("gr", "fs"), "tp"),
        P(("gr", "fs")),
    )
    return jax.shard_map(
        functools.partial(body, mesh.shape["gr"], mesh.shape["fs"], mesh.shape["tp"]),
        mesh=mesh,
        in_specs=placed,
        out_specs=(P(None, ("gr", "tp")), P(None, ("gr", "tp")), P(("gr", "fs", "tp"), None)),
        check_vma=False,
    )
```

```python
import functools

import jax
import jax.numpy as jnp
from jax import lax
from jax.experimental import pallas as pl
from jax.experimental.pallas import tpu as pltpu
from jax.sharding import PartitionSpec as P

MESH = pl.DeviceIdType.MESH
CHUNK = 32
TILE = 256
SPLIT = 4


def pair_share(count, width):
    share = []
    for eighths in (count * 10 // 8, count * 11 // 8):
        share.append((eighths // 8, eighths % 8 * (width // 8)))
    return share


def kernel(G, F, T, tok_in, gain_in, up_in, down_in, up_full, down_full, part,
           wide, narrow, raw, nrm, hid, stage,
           recv, dup, cross, cross_down, sendl, sendr, sendy, send0, tok_recv, tok_send,
           part_recv, part_send, local_sem, load_sem, ready):
    gr, f, tp = lax.axis_index("gr"), lax.axis_index("fs"), lax.axis_index("tp")
    full = (up_full, down_full)
    A = F // 2
    a, y = f // 2, f % 2
    mate = a * 2 + 1 - y
    R = up_in.shape[0]
    D, W = up_full.shape
    tok = tok_in.shape[0]
    CH = min(CHUNK, R)
    C = R // CH
    NQ = G * C
    share = pair_share(NQ, W)
    K = G * T
    k = gr * T + tp
    weights = (up_in, down_in)

    def at_k(kk):
        return (kk // T, f, kk % T)

    def load(m, c):
        rows = pl.ds(c * CH, CH) if m == 0 else pl.ds(0, R)
        return pltpu.make_async_copy(weights[m].at[rows], wide.at[m, rows], load_sem.at[c if m == 0 else C])

    load(0, 0).start()
    barrier = pltpu.get_barrier_semaphore()

    @pl.when(a < A - 1)
    def _():
        pl.semaphore_signal(barrier, inc=1, device_id=(gr, f + 2, tp), device_id_type=MESH)

    @pl.when(y == 0)
    def _():
        pl.semaphore_signal(barrier, inc=1, device_id=(gr, mate, tp), device_id_type=MESH)

    for kk in range(1, K):
        @pl.when(kk > k)
        def _():
            pl.semaphore_signal(barrier, inc=1, device_id=at_k(kk), device_id_type=MESH)

    token_load = pltpu.make_async_copy(tok_in, raw, local_sem.at[0])
    partners = (a > 0).astype(jnp.int32) + y + k

    @pl.when(partners > 0)
    def _():
        pl.semaphore_wait(barrier, partners)

    @pl.when(a > 0)
    def _():
        pl.semaphore_signal(ready.at[0], inc=1, device_id=(gr, f - 2, tp), device_id_type=MESH)

    @pl.when(y == 1)
    def _():
        pl.semaphore_signal(ready.at[1], inc=1, device_id=(gr, mate, tp), device_id_type=MESH)

    for kk in range(K - 1):
        @pl.when(kk < k)
        def _():
            pl.semaphore_signal(ready.at[1 + k], inc=1, device_id=at_k(kk), device_id_type=MESH)

    for c in range(1, C):
        load(0, c).start()

    def rows_of(origin, g, c):
        return pl.ds(pl.multiple_of(g * (F * R) + origin * R + c * CH, CH), CH)

    home = k // G == tp

    def cast(m, c):
        rows = pl.ds(c * CH, CH)
        if m == 0 or c == 0:
            load(m, c).wait()
        value = wide[m, rows, :]
        if m == 0:
            value = value * column[c * CH:(c + 1) * CH]
        value = value.astype(jnp.bfloat16)
        narrow[m, rows, :] = value
        for b in range(G):
            @pl.when(tp * G + b == k)
            def _():
                full[m][rows_of(f, gr, c), :] = value[:, b * W:(b + 1) * W]

    batch = 2 if C % 2 == 0 else 1

    def slot(q):
        return jnp.where(q < C, q, C + (q - C) // batch)

    def hand(m, b, c):
        kk = tp * G + b
        q = ((gr - kk // T + G) % G) * C + c

        @pl.when(kk != k)
        def _():
            copy = pltpu.make_async_remote_copy(
                src_ref=narrow.at[m, pl.ds(c * CH, CH), pl.ds(b * W, W)],
                dst_ref=full[m].at[rows_of(f, gr, c)],
                send_sem=send0.at[0], recv_sem=recv.at[m, a, slot(q)],
                device_id=at_k(kk), device_id_type=MESH)
            copy.start()

    mine = pl.ds(pl.multiple_of(k * tok, 16), tok)

    def tokens():
        for d in range(1, K):
            pltpu.make_async_remote_copy(
                src_ref=nrm.at[mine], dst_ref=nrm.at[mine],
                send_sem=tok_send.at[0], recv_sem=tok_recv.at[0],
                device_id=at_k((k + d) % K), device_id_type=MESH).start()

    def normalize(i, carry):
        values = raw[pl.ds(pl.multiple_of(i * 16, 16), 16), :].astype(jnp.float32)
        center = jnp.mean(values, axis=-1, keepdims=True)
        moved = values - center
        spread = jnp.mean(jnp.square(moved), axis=-1, keepdims=True)
        nrm[pl.ds(pl.multiple_of(k * tok + i * 16, 16), 16), :] = (
            moved * lax.rsqrt(spread + 1e-05)).astype(jnp.bfloat16)
        return carry

    rowed = lax.broadcasted_iota(jnp.int32, (R, R), 0) == lax.broadcasted_iota(jnp.int32, (R, R), 1)
    column = jnp.sum(jnp.where(rowed, gain_in[...], 0.0), axis=1, keepdims=True)

    def chunk(m, origin, q, columns):
        rows = rows_of(origin, (gr + q // C) % G, q % C)
        return full[m].at[rows, pl.ds(columns[0], columns[1] - columns[0])]

    def landing(m, origin_a, side, q):
        if side == "line":
            return recv.at[m, origin_a, slot(q)]
        if side == "pair":
            return dup.at[m, origin_a]
        return cross.at[0] if m == 0 else cross_down.at[origin_a, q // C]

    whole = (0, W)

    def send(m, origin, q, sem, side, target, columns=whole):
        ref = chunk(m, origin, q, columns)
        pltpu.make_async_remote_copy(
            src_ref=ref, dst_ref=ref, send_sem=sem.at[0], recv_sem=landing(m, origin // 2, side, q),
            device_id=(gr, target, tp), device_id_type=MESH).start()

    def await_rows(ref, count, sem):
        if count > 0:
            rows = ref.at[pl.ds(0, count)]
            if len(ref.shape) == 2 and count % 8:
                rows = ref.at[pl.ds(0, 2 * count), pl.ds(0, ref.shape[1] // 2)]
            pltpu.make_async_copy(rows, rows, sem).wait()

    def arrived(m, origin, q):
        sem = landing(m, origin // 2, "line", q)

        @pl.when(q < C)
        def _():
            ref = chunk(m, origin, q, whole)
            pltpu.make_async_copy(ref, ref, sem).wait()

        @pl.when(jnp.logical_and(q >= C, (q - C) % batch == 0))
        def _():
            await_rows(full[m], batch * CH, sem)

    def left(m, origin, q, side="line", columns=whole):
        @pl.when(a > 0)
        def _():
            send(m, origin, q, sendl, side, f - 2, columns)

    def right(m, origin, q, side="line", columns=whole):
        @pl.when(a < A - 1)
        def _():
            send(m, origin, q, sendr, side, f + 2, columns)

    def loop(low, high, step):
        def go(i, carry):
            step(i)
            return carry
        if high > low:
            lax.fori_loop(low, high, go, 0)

    def over_line(m):
        pf, shared = share[m]
        first = pf + (shared > 0)
        return ([(0, pf, ())] if pf else []) + ([(pf, first, (shared, W))] if shared else []), (first, C, whole)

    def over_pair(m):
        pf, shared = share[m]
        return ([(0, pf, whole)] if pf else []) + ([(pf, pf + 1, (0, shared))] if shared else [])

    def across(m, origin, q, columns):
        if columns:
            send(m, origin, q, sendy, "cross", mate, columns)

    def own_across(m, q, columns, pair=True):
        if pair and columns[:1] != (0,):
            send(m, f, q, sendy, "pair", mate, (0, columns[0]) if columns else whole)
        across(m, f, q, columns)

    def own_chunk(m, q, columns, pair=True):
        left(m, f, q)
        right(m, f, q)
        own_across(m, q, columns, pair)

    def own(m):
        def near(columns):
            def step(q):
                @pl.when(jnp.logical_not(home))
                def _():
                    arrived(m, f, q)
                    if m == 0:
                        own_chunk(m, q, columns)
                if m > 0:
                    own_chunk(m, q, columns, False)
            return step

        def far(q):
            arrived(m, f, q)
            own_chunk(m, q, whole)

        shared, rest = over_line(m)
        if m == 0:
            for low, high, columns in shared:
                loop(low, high, near(columns))
            loop(rest[0], rest[1], near(whole))
            loop(C, NQ, far)
        else:
            for low, high, columns in over_pair(m):
                def step(q):
                    @pl.when(jnp.logical_not(home))
                    def _():
                        arrived(m, f, q)
                    send(m, f, q, sendy, "pair", mate, columns)
                loop(low, high, step)

            loop(C, NQ, far)

            def step(columns):
                def go(q):
                    own_chunk(m, q, columns, False)
                return go
            for low, high, columns in shared:
                if columns:
                    loop(low, high, step(columns))
            loop(rest[0], rest[1], near(whole))
            for low, high, columns in shared:
                if not columns:
                    loop(low, high, step(columns))

    def mated(m):
        await_rows(full[m], pair_rows(m), dup.at[m, a])
        for low, high, columns in over_pair(m):
            def step(q):
                left(m, mate, q, "pair", columns)
                right(m, mate, q, "pair", columns)
            loop(low, high, step)

    def line(m, s, between=None, eager=None, closing=None):
        below, above = a - 1 - s, a + 1 + s

        def both(side, columns):
            sent = columns if side == "pair" else whole

            def pass_on(origin, q, onward):
                if side == "line":
                    arrived(m, origin, q)
                onward(m, origin, q, side, sent)
                if side == "line":
                    across(m, origin, q, columns)

            def step(q):
                mine_y = y if side == "line" else 1 - y

                @pl.when(below >= 0)
                def _():
                    pass_on(below * 2 + mine_y, q, right)

                @pl.when(above < A)
                def _():
                    pass_on(above * 2 + mine_y, q, left)
            return step

        shared, rest = over_line(m)
        if m == 0:
            for low, high, columns in shared:
                loop(low, high, both("line", columns))
            loop(rest[0], rest[1], both("line", whole))
            loop(C, NQ, both("line", whole))
        else:
            loop(C, NQ, both("line", whole))
            if between is not None:
                between()
            for low, high, columns in shared:
                if columns:
                    loop(low, high, both("line", columns))
            loop(rest[0], rest[1], both("line", whole))
            if eager is not None:
                eager()
            for low, high, columns in shared:
                if not columns:
                    loop(low, high, both("line", columns))
        if closing is not None:
            closing()
        for origin_a in (below, above):
            @pl.when(jnp.logical_and(origin_a >= 0, origin_a < A))
            def _():
                await_rows(full[m], pair_rows(m), dup.at[m, origin_a])
        for low, high, columns in over_pair(m):
            loop(low, high, both("pair", columns))

    def pair_rows(m):
        pf, shared = share[m]
        return pf * CH + CH * shared // W

    def settle_down(origin_a, gi):
        @pl.when(gi == 0)
        def _():
            await_rows(down_full, C * CH - pair_rows(1), cross_down.at[origin_a, 0])

        @pl.when(gi > 0)
        def _():
            await_rows(down_full, C * CH, cross_down.at[origin_a, gi])

    def sharing(c):
        pf, shared = share[0]
        return () if c < pf else (shared if c == pf else 0, W)

    for c in range(C):
        cast(0, c)

        @pl.when(home)
        def _():
            left(0, f, c)

            @pl.when(y == 1)
            def _():
                own_across(0, c, sharing(c))

    load(1, 0).start()
    token_load.start()

    def meet(kk):
        @pl.when(kk > k)
        def _():
            pl.semaphore_wait(ready.at[1 + kk], 1)

    for b in range(G):
        meet(tp * G + b)
    for c in range(C):
        for b in range(G):
            hand(0, b, c)

    @pl.when(y == 0)
    def _():
        pl.semaphore_wait(ready.at[1], 1)

        @pl.when(home)
        def _():
            for c in range(C):
                own_across(0, c, sharing(c))

    @pl.when(a < A - 1)
    def _():
        pl.semaphore_wait(ready.at[0], 1)

        @pl.when(home)
        def _():
            for c in range(C):
                right(0, f, c)

    own(0)
    token_load.wait()
    lax.fori_loop(0, tok // 16, normalize, 0)
    for c in range(C):
        cast(1, c)
        for b in range(G):
            hand(1, b, c)
    for kk in range(1, K):
        @pl.when(kk // G != tp)
        def _():
            meet(kk)
    tokens()
    mated(0)
    loop(0, A - 2, lambda s: line(0, s))
    own(1)
    line(0, A - 2)
    mated(1)
    line(1, 0)

    await_rows(up_full, A * (NQ * CH - pair_rows(0)), cross.at[0])
    await_rows(nrm, (K - 1) * tok, tok_recv.at[0])

    tile = min(TILE, W)

    def lift(j):
        columns = pl.ds(pl.multiple_of(j * tile, tile), tile)
        lifted = jnp.maximum(jnp.dot(nrm[...], up_full[:, columns], preferred_element_type=jnp.float32), 0.0)
        hid[:, columns] = (lifted * lifted).astype(jnp.bfloat16)
    loop(0, W // tile, lift)

    halves = 2 if R % 128 == 0 else 1

    def part_copy(d, block, columns):
        target = (k + d) % K
        return pltpu.make_async_remote_copy(
            src_ref=stage.at[block, pl.ds(pl.multiple_of(target * tok, 16), tok), columns],
            dst_ref=part.at[d - 1, block, :, columns],
            send_sem=part_send.at[0], recv_sem=part_recv.at[0],
            device_id=at_k(target), device_id_type=MESH)

    def multiply(block, rows, columns):
        value = lax.dot_general(hid[...], down_full[rows, :], (((1,), (1,)), ((), ())),
                                preferred_element_type=jnp.float32)
        stage[block, :, columns] = value.astype(jnp.bfloat16)
        for d in range(1, K):
            part_copy(d, block, columns).start()
        part[K - 1, block, :, columns] = stage[block, mine, columns]

    far = jnp.where(2 * a < A, A - 1, 0)

    def lower(origin_a, gi):
        settle_down(origin_a, gi)
        g = (gr + gi) % G
        rows = pl.ds(pl.multiple_of(g * (F * R) + origin_a * (2 * R), 2 * R), 2 * R)
        multiply(origin_a * G + g, rows, pl.ds(0, 2 * R))

    def lower_half(origin_a, side):
        rows = pl.ds(pl.multiple_of(gr * (F * R) + (origin_a * 2 + side) * R, R), R)
        multiply(origin_a * G + gr, rows, pl.ds(pl.multiple_of(side * R, R), R))

    def at_far(step):
        for end in (0, A - 1):
            @pl.when(far == end)
            def _():
                step(end)

    def early():
        if halves == 2:
            at_far(lambda origin_a: lower_half(origin_a, y))

    def late():
        if halves == 2:
            settle_down(far, 0)
            at_far(lambda origin_a: lower_half(origin_a, 1 - y))
        else:
            lower(far, 0)

    def lower_ring(s, last=True):
        def blocks(origin_a):
            loop(0, G - 1, lambda i: lower(origin_a, G - 1 - i))

            if last:
                @pl.when(origin_a != far)
                def _():
                    lower(origin_a, 0)

        @pl.when(a - 1 - s >= 0)
        def _():
            blocks(a - 1 - s)

        @pl.when(a + 1 + s < A)
        def _():
            blocks(a + 1 + s)

    loop(0, G, lambda i: lower(a, G - 1 - i))
    loop(1, A - 2, lambda s: line(1, s, between=lambda: lower_ring(s - 1)))
    line(1, A - 2, between=lambda: lower_ring(A - 3), eager=lambda: lower_ring(A - 2, False), closing=early)
    late()

    await_rows(nrm, (K - 1) * tok, tok_send.at[0])
    pairs = pair_rows(0) + pair_rows(1)
    await_rows(up_full, 2 * NQ * CH, sendy.at[0])
    for _ in range(A - 1):
        await_rows(up_full, 2 * NQ * CH - pairs, sendy.at[0])

    def drain(sem, rows):
        def step(i, carry):
            await_rows(up_full, rows, sem.at[0])
            return carry
        return step
    lax.fori_loop(0, jnp.where(a > 0, A - a, 0), drain(sendl, 2 * NQ * CH + pairs), 0)
    lax.fori_loop(0, jnp.where(a < A - 1, a + 1, 0), drain(sendr, 2 * NQ * CH + pairs), 0)
    lax.fori_loop(0, jnp.where(home, G - 1, G), drain(send0, 2 * R), 0)
    await_rows(part, K - 1, part_recv.at[0])
    await_rows(part, K - 1, part_send.at[0])


def finish(G, F, up_held, down_held, parts, up_out, down_out, out_ref, summed, sems, out_sem):
    def out(m, i):
        source, target = ((up_held, up_out), (down_held, down_out))[m]
        size = source.shape[0] // SPLIT
        rows = pl.ds(i * size, size)
        return pltpu.make_async_copy(source.at[rows], target.at[rows], sems.at[m, i])

    for m in range(2):
        for i in range(SPLIT):
            out(m, i).start()
    K, blocks, _, wide = parts.shape
    D = out_ref.shape[1]
    for block in range(blocks):
        total = parts[0, block].astype(jnp.float32)
        for i in range(1, K):
            total += parts[i, block].astype(jnp.float32)
        begin = (block % G) * (D // G) + (block // G) * wide
        summed[:, begin:begin + wide] = total.astype(jnp.bfloat16)
    tokens_out = pltpu.make_async_copy(summed, out_ref, out_sem.at[0])
    tokens_out.start()
    for m in range(2):
        for i in range(SPLIT):
            out(m, i).wait()
    tokens_out.wait()


def body(G, F, T, prompt_tokens, up_master, down_master, norm_gain):
    R, width = up_master.shape
    tok = prompt_tokens.shape[0]
    D, W = R * G * F, width // G
    A, K = F // 2, G * T
    C = R // min(CHUNK, R)
    NQ = G * C
    bf16 = jnp.bfloat16
    any_space = pl.BlockSpec(memory_space=pl.ANY)
    vmem_space = pl.BlockSpec(memory_space=pltpu.VMEM)
    dma = pltpu.SemaphoreType.DMA
    up_held, down_held, parts = pl.pallas_call(
        functools.partial(kernel, G, F, T),
        name="handoff",
        out_shape=(
            pltpu.MemorySpace.VMEM((D, W), bf16),
            pltpu.MemorySpace.VMEM((D, W), bf16),
            pltpu.MemorySpace.VMEM((K, A * G, tok, 2 * R), bf16),
        ),
        in_specs=[any_space, vmem_space, any_space, any_space],
        out_specs=(vmem_space,) * 3,
        scratch_shapes=[
            pltpu.VMEM((2, R, width), jnp.float32),
            pltpu.VMEM((2, R, width), bf16),
            pltpu.VMEM((tok, D), bf16),
            pltpu.VMEM((K * tok, D), bf16),
            pltpu.VMEM((K * tok, W), bf16),
            pltpu.VMEM((A * G, K * tok, 2 * R), bf16),
            dma((2, A, C + (NQ - C) // (2 if C % 2 == 0 else 1))), dma((2, A)), dma((1,)), dma((A, G)),
            dma((1,)), dma((1,)), dma((1,)), dma((1,)), dma((1,)), dma((1,)),
            dma((1,)), dma((1,)), dma((1,)), dma((C + 1,)), pltpu.SemaphoreType.REGULAR((K + 1,)),
        ],
        compiler_params=pltpu.CompilerParams(
            collective_id=0, has_side_effects=True, vmem_limit_bytes=41 * 1024 * 1024),
    )(prompt_tokens, norm_gain.reshape(1, R), up_master, down_master)
    return pl.pallas_call(
        functools.partial(finish, G, F),
        name="finish",
        out_shape=(
            jax.ShapeDtypeStruct((D, W), bf16),
            jax.ShapeDtypeStruct((D, W), bf16),
            jax.ShapeDtypeStruct((tok, D), bf16),
        ),
        in_specs=[vmem_space] * 3,
        out_specs=(any_space, any_space, any_space),
        scratch_shapes=[pltpu.VMEM((tok, D), bf16), dma((2, SPLIT)), dma((1,))],
        compiler_params=pltpu.CompilerParams(vmem_limit_bytes=16 * 1024 * 1024),
    )(up_held, down_held, parts)


def solution(mesh):
    placed = (
        P(("gr", "fs", "tp"), None),
        P(("gr", "fs"), "tp"),
        P(("gr", "fs"), "tp"),
        P(("gr", "fs")),
    )
    return jax.shard_map(
        functools.partial(body, mesh.shape["gr"], mesh.shape["fs"], mesh.shape["tp"]),
        mesh=mesh,
        in_specs=placed,
        out_specs=(P(None, ("gr", "tp")), P(None, ("gr", "tp")), P(("gr", "fs", "tp"), None)),
        check_vma=False,
    )
```
